32 devices in a mesh: rep: 2 (over core), fs: 8 (over z, y), tp: 2 (over x).
Axes of the slice: x: 2, y: 2, z: 4, core: 2. Of those that a mesh axis runs over, the one named last changes fastest.
Arguments:
- tokens: bfloat16 [16, 768, 2048], P(('rep', 'fs')), may hold values from -6 to 6
- mixer_gain: float32 [2048], replicated, may hold values from 0.1 to 1.9
- value_weight: float32 [2048, 4, 512], P('fs', None, 'tp'), may hold values from -0.125 to 0.125
- value_scale: float32 [4, 512], P(None, 'tp'), may hold values from 0.5 to 2
- gate_weight: float32 [2048, 4, 512], P('fs', None, 'tp'), may hold values from -0.125 to 0.125
- gate_scale: float32 [4, 512], P(None, 'tp'), may hold values from 0.5 to 2
- pool_weight: float32 [4, 512, 512], P(None, 'fs', 'tp'), may hold values from -0.25 to 0.25
- pool_scale: float32 [4, 512], P(None, 'tp'), may hold values from 0.5 to 2
- channel_gain: float32 [2048], replicated, may hold values from 0.1 to 1.9
- up_weight: float32 [2048, 4096], P('fs', 'tp'), may hold values from -0.125 to 0.125
- up_scale: float32 [4096], P('tp'), may hold values from 0.5 to 2
- down_weight: float32 [4096, 2048], P('tp', 'fs'), may hold values from -0.09375 to 0.09375
- down_scale: float32 [2048], P('fs'), may hold values from 0.5 to 2
Outputs:
- layer_out: bfloat16 [16, 768, 2048], P(('rep', 'fs'), 'tp')
The draws below stay inside these ranges and needn't reach their ends.
All inputs are finite; a program needn't handle non-finite values.
Results may differ from the reference program's by a relative error of at most 0.015.
Values may be sent and summed in bfloat16 or wider, within the bound.
A program may use at most 64 MiB of HBM per device.

```python
import math
import jax
import jax.numpy as jnp
from jax import lax

D = 2048
GROUPS = 4
GROUP_WIDTH = 512
FF = 4096
SEQ_LEN = 768
SEQS = 16
N_TP = 2


def levels(rng, dims, pieces, low, high):
    loudness, own = 1.0, jax.random.fold_in(rng, 6)
    for dim, parts in pieces:
        steps = jnp.exp(jax.random.uniform(jax.random.fold_in(own, dim), (parts,), jnp.float32, low / len(pieces), high / len(pieces)))
        loudness = loudness * jnp.repeat(steps, dims[dim] // parts).reshape([-1 if axis == dim else 1 for axis in range(len(dims))])
    return loudness


def normal_values(own_key, dims, scale, limit, shards=(), dtype=jnp.bfloat16):
    loudness = levels(own_key, dims, shards, -0.22, 0.18) if shards else 1.0
    values = jax.random.normal(own_key, dims, jnp.float32) * scale * loudness
    return jnp.minimum(jnp.maximum(values, -limit), limit).astype(dtype)


def setup_inputs(seed: int = 0) -> dict:
    seeds = jax.random.split(jax.random.key(seed), 14)
    tokens = normal_values(seeds[0], (SEQS, SEQ_LEN, D), 1.0, 6.0, ((0, 16),))
    mixer_gain = jnp.clip(1.0 + 0.18 * jax.random.normal(seeds[1], (D,), jnp.float32), 0.1, 1.9)
    value_weight = normal_values(seeds[2], (D, GROUPS, GROUP_WIDTH), D ** -0.5, 0.125, ((0, 8), (2, 2)), jnp.float32)
    value_scale = jnp.clip(jnp.exp(math.log(2.0) - 1.3862944 * jax.random.uniform(seeds[3], (GROUPS, GROUP_WIDTH), jnp.float32) ** levels(seeds[3], (GROUPS, GROUP_WIDTH), ((1, 2),), -0.2, 0.2)), 0.5, 2.0)
    gate_weight = normal_values(seeds[4], (D, GROUPS, GROUP_WIDTH), D ** -0.5, 0.125, ((0, 8), (2, 2)), jnp.float32)
    gate_scale = jnp.clip(jnp.exp(math.log(2.0) - 1.3862944 * jax.random.uniform(seeds[5], (GROUPS, GROUP_WIDTH), jnp.float32) ** levels(seeds[5], (GROUPS, GROUP_WIDTH), ((1, 2),), -0.2, 0.2)), 0.5, 2.0)
    pool_weight = normal_values(seeds[6], (GROUPS, GROUP_WIDTH, GROUP_WIDTH), GROUP_WIDTH ** -0.5, 0.25, ((1, 8), (2, 2)), jnp.float32)
    pool_scale = jnp.clip(jnp.exp(math.log(2.0) - 1.3862944 * jax.random.uniform(seeds[7], (GROUPS, GROUP_WIDTH), jnp.float32) ** levels(seeds[7], (GROUPS, GROUP_WIDTH), ((1, 2),), -0.2, 0.2)), 0.5, 2.0)
    channel_gain = jnp.clip(1.0 + 0.18 * jax.random.normal(seeds[8], (D,), jnp.float32), 0.1, 1.9)
    up_weight = normal_values(seeds[9], (D, FF), D ** -0.5, 0.125, ((0, 8), (1, 2)), jnp.float32)
    up_scale = jnp.clip(jnp.exp(math.log(2.0) - 1.3862944 * jax.random.uniform(seeds[10], (FF,), jnp.float32) ** levels(seeds[10], (FF,), ((0, 2),), -0.2, 0.2)), 0.5, 2.0)
    down_weight = normal_values(seeds[11], (FF, D), FF ** -0.5, 0.09375, ((0, 2), (1, 8)), jnp.float32)
    down_scale = jnp.clip(jnp.exp(math.log(2.0) - 1.3862944 * jax.random.uniform(seeds[12], (D,), jnp.float32) ** levels(seeds[12], (D,), ((0, 8),), -0.2, 0.2)), 0.5, 2.0)
    return dict(tokens=tokens, mixer_gain=mixer_gain, value_weight=value_weight, value_scale=value_scale, gate_weight=gate_weight, gate_scale=gate_scale, pool_weight=pool_weight, pool_scale=pool_scale, channel_gain=channel_gain, up_weight=up_weight, up_scale=up_scale, down_weight=down_weight, down_scale=down_scale)


def norm_rows(values, gain):
    floats = values.astype(jnp.float32)
    return floats * lax.rsqrt(lax.optimization_barrier(jnp.mean(floats * floats, axis=-1, keepdims=True)) + 1e-06) * gain

def pool_excess(value):
    floats = value.astype(jnp.float32)
    seq_length = floats.shape[1]
    running = floats
    results = []
    for group in range(floats.shape[2]):
        span = 2 ** group
        shifted = jnp.pad(running, ((0, 0), (span, 0), (0, 0), (0, 0)))[:, :seq_length]
        running = running + shifted
        counts = jnp.minimum(jnp.arange(1, seq_length + 1), 2 * span).astype(jnp.float32)
        results.append(running[:, :, group, :] / counts[None, :, None] - floats[:, :, group, :])
    return jnp.stack(results, axis=2)

def rounded(values):
    return lax.optimization_barrier(values.astype(jnp.bfloat16)).astype(jnp.float32)

def reference(tokens, mixer_gain, value_weight, value_scale, gate_weight, gate_scale, pool_weight, pool_scale, channel_gain, up_weight, up_scale, down_weight, down_scale):
    seq_count, seq_length, model_width = tokens.shape
    row_count = seq_count * seq_length
    normed = norm_rows(tokens, mixer_gain).astype(jnp.bfloat16).reshape(row_count, model_width)
    value = jnp.dot(normed, value_weight.astype(jnp.bfloat16).reshape(model_width, -1), preferred_element_type=jnp.float32)
    value = (value * value_scale.reshape(-1)).astype(jnp.bfloat16).reshape(seq_count, seq_length, GROUPS, GROUP_WIDTH)
    gate = jnp.dot(normed, gate_weight.astype(jnp.bfloat16).reshape(model_width, -1), preferred_element_type=jnp.float32)
    gate = (gate * gate_scale.reshape(-1)).reshape(seq_count, seq_length, GROUPS, GROUP_WIDTH)
    excess = pool_excess(value).astype(jnp.bfloat16)
    pooled = jnp.einsum('slgc,gce->slge', excess.astype(jnp.float32), pool_weight.astype(jnp.bfloat16).astype(jnp.float32)) * pool_scale
    merged = (jax.nn.sigmoid(gate) * pooled).astype(jnp.bfloat16)
    middle = tokens.reshape(row_count, model_width).astype(jnp.float32) + merged.reshape(row_count, model_width).astype(jnp.float32)
    normed_two = norm_rows(middle, channel_gain).astype(jnp.bfloat16)
    upward = jnp.dot(normed_two, up_weight.astype(jnp.bfloat16), preferred_element_type=jnp.float32) * up_scale
    hidden = jnp.square(jax.nn.relu(upward)).astype(jnp.bfloat16)
    down_matrix = down_weight.astype(jnp.bfloat16)
    hidden_block = FF // N_TP
    summed = jnp.zeros((row_count, model_width), jnp.float32)
    for member in range(N_TP):
        part = hidden[:, member * hidden_block:(member + 1) * hidden_block]
        rows_part = down_matrix[member * hidden_block:(member + 1) * hidden_block]
        summed = summed + rounded(jnp.dot(part, rows_part, preferred_element_type=jnp.float32) * down_scale)
    return (middle + summed).astype(jnp.bfloat16).reshape(seq_count, seq_length, model_width)
```

```python
import functools

import jax
import jax.numpy as jnp
from jax import lax
from jax.experimental import pallas as pl
from jax.experimental.pallas import tpu as pltpu
from jax.sharding import PartitionSpec as P

NY = 2
ACROSS, SIBLING = 2, 3


class Gather:
    def __init__(self, sizes, bufs, sems):
        self.nf = sizes["fs"]
        self.nz = self.nf // NY
        self.rep, self.place, self.tp = lax.axis_index("rep"), lax.axis_index("fs"), lax.axis_index("tp")
        self.z, self.y = self.place // NY, self.place % NY
        self.mixed, self.hide, self.show, self.stage = bufs
        self.send_sem, self.recv_sem = sems
        self.nm, self.nh = self.mixed.shape[0], self.hide.shape[0]
        self.subs = 4
        self.count = self.nm + self.nh + self.subs

    def device(self, way):
        rep, place = self.rep, self.place
        if isinstance(way, int) and way == ACROSS:
            place = self.z * NY + 1 - self.y
        elif isinstance(way, int) and way == SIBLING:
            rep = 1 - rep
        else:
            place = place + NY * (2 * way - 1)
        return {"rep": rep, "fs": place, "tp": self.tp}

    def partner(self):
        return {"rep": self.rep, "fs": self.place, "tp": 1 - self.tp}

    def half_of(self, p):
        j, q = p // 2, p % 2
        return 2 * j + (self.tp if q == 0 else 1 - self.tp)

    def piece(self, p, k, half):
        if isinstance(p, int) and p < self.nm:
            part = self.mixed.shape[2] // 2
            return self.mixed.at[self.half_of(p), k, pl.ds(pl.multiple_of(half * part, 16), part), :]
        if isinstance(p, int) and p < self.nm + self.nh:
            part = self.hide.shape[2] // 2
            return self.hide.at[p - self.nm, k, pl.ds(pl.multiple_of(half * part, 16), part), :]
        part = self.show.shape[1] // (2 * self.subs)
        sub = p - self.nm - self.nh
        return self.show.at[k, pl.ds(pl.multiple_of((2 * sub + half) * part, 16), part), :]

    def copy(self, p, k, way, half=None, src=None):
        half = self.rep if half is None else half
        sibling = isinstance(way, int) and way == SIBLING
        return pltpu.make_async_remote_copy(
            src_ref=self.piece(p, k, half) if src is None else src,
            dst_ref=self.piece(p, k, half),
            send_sem=self.send_sem.at[way, p, k],
            recv_sem=self.recv_sem.at[1 if sibling else 0, p, k],
            device_id=self.device(way),
            device_id_type=pl.DeviceIdType.MESH,
        )

    def inside(self, z):
        return (z >= 0) & (z < self.nz)

    def wide(self, p, zs):
        return ((zs == 0) | (zs == self.nz - 1)) & (self.rep == p % 2)

    def greet(self):
        sem = pltpu.get_barrier_semaphore()

        def signal(device):
            pl.semaphore_signal(sem, inc=1, device_id=device, device_id_type=pl.DeviceIdType.MESH)

        signal(self.device(ACROSS))
        signal(self.device(SIBLING))
        signal(self.partner())
        pl.when(self.z > 0)(lambda: signal(self.device(0)))
        pl.when(self.z < self.nz - 1)(lambda: signal(self.device(1)))

    def meet(self):
        ends = (self.z > 0).astype(jnp.int32) + (self.z < self.nz - 1).astype(jnp.int32)
        pl.semaphore_wait(pltpu.get_barrier_semaphore(), 3 + ends)

    def each(self, phase, body):
        if phase < self.nm + self.nh:
            body(phase)
        else:
            pl.loop(0, self.subs)(lambda sub: body(self.nm + self.nh + sub))

    def source(self, p):
        if not (isinstance(p, int) and p < self.nm and p % 2 == 0):
            return None
        part = self.stage.shape[1] // 2
        rows = pl.ds(pl.multiple_of(self.rep * part, 16), part)
        return self.stage.at[2 * self.tp + p // 2, rows, :]

    def own(self, phase):
        def body(p):
            src = self.source(p)

            @pl.loop(0, 2)
            def _(way):
                there = self.inside(self.z + 2 * way - 1)
                pl.when(there)(lambda: self.copy(p, self.place, way, src=src).start())

            self.copy(p, self.place, ACROSS, src=src).start()

        self.each(phase, body)

    def along(self, phase, d):
        @pl.loop(0, 2)
        def _(way):
            step = 2 * way - 1
            zs = self.z - step * d

            @pl.when(self.inside(zs))
            def _():
                k = zs * NY + self.y

                def body(p):
                    self.copy(p, k, ACROSS).wait_recv()
                    pl.when(self.inside(self.z + step))(lambda: self.copy(p, k, way).start())
                    pl.when(jnp.logical_not(self.wide(p, zs)))(lambda: self.copy(p, k, ACROSS).start())
                    self.copy(p, k, SIBLING).start()

                self.each(phase, body)

    def across(self, phase, d):
        if d == 0:
            k = self.z * NY + 1 - self.y
            way = (self.z == 0).astype(jnp.int32)

            def first(p):
                self.copy(p, k, ACROSS).wait_recv()
                pl.when(self.wide(p, self.z))(lambda: self.copy(p, k, way).start())
                self.copy(p, k, SIBLING).start()

            self.each(phase, first)
            return

        @pl.loop(0, 2)
        def _(way):
            step = 2 * way - 1
            zs = self.z - step * d

            @pl.when(self.inside(zs))
            def _():
                k = zs * NY + 1 - self.y

                def body(p):
                    self.copy(p, k, ACROSS).wait_recv()
                    onward = self.wide(p, zs) & self.inside(self.z + step)
                    pl.when(onward)(lambda: self.copy(p, k, way).start())
                    self.copy(p, k, SIBLING).start()

                self.each(phase, body)

    def wait_sibling(self, phase, k):
        self.each(phase, lambda p: self.copy(p, k, SIBLING, half=1 - self.rep).wait_recv())

    def ready(self, phase):
        @pl.loop(0, self.nf)
        def _(k):
            pl.when(k != self.place)(lambda: self.wait_sibling(phase, k))

    def drain(self, phase):
        def body(p):
            src = self.source(p)

            @pl.loop(0, self.nf)
            def _(k):
                zs, mine = k // NY, k % NY == self.y
                wide = self.wide(p, zs)
                here = zs == self.z

                @pl.loop(0, 2)
                def _(way):
                    step = 2 * way - 1
                    away = here | (step * (self.z - zs) > 0)
                    sent = self.inside(self.z + step) & away & (mine | wide)
                    pl.when(sent)(lambda: self.copy(p, k, way).wait_send())

                pl.when(mine & (here | jnp.logical_not(wide)))(lambda: self.copy(p, k, ACROSS).wait_send())
                pl.when(k != self.place)(lambda: self.copy(p, k, SIBLING).wait_send())

        self.each(phase, body)


def layer_kernel(sizes, *refs):
    mixer_gain, value_scale, gate_scale, pool_scale, channel_gain, up_scale, down_scale = refs[:7]
    tokens_far, value_far, gate_far, pool_far, up_far, down_far, out = refs[7:14]
    mixed, hide, show, stage = refs[14:18]
    tokens, value_near, gate_near, pool_near, up_near, down_near = refs[18:24]
    normed, excess, merged, merged_in, hidden, part_out, part_own, part_in = refs[24:32]
    send_sem, recv_sem, load_sem, swap_send, swap_recv, keep_sem, pair_send, pair_recv = refs[32:]
    g = Gather(sizes, (mixed, hide, show, stage), (send_sem, recv_sem))
    rows, width = tokens.shape
    groups, cells, local = pool_near.shape
    depth = value_near.shape[0]
    half = rows // 2
    inner = hidden.shape[1]
    member, rep, place = g.tp, g.rep, g.place
    nm, nh = g.nm, g.nh
    last = nm + nh
    each_group = nm // 2

    loads = [
        pltpu.make_async_copy(far, near, load_sem.at[i])
        for i, (far, near) in enumerate(
            (
                (value_far, value_near),
                (gate_far, gate_near),
                (pool_far, pool_near),
                (tokens_far, tokens),
                (up_far, up_near),
                (down_far, down_near),
            )
        )
    ]

    def remote(source, target, send, recv):
        return pltpu.make_async_remote_copy(
            src_ref=source,
            dst_ref=target,
            send_sem=send,
            recv_sem=recv,
            device_id=g.partner(),
            device_id_type=pl.DeviceIdType.MESH,
        )

    def swap(j, part):
        size = stage.shape[1] // 2
        cut = pl.ds(pl.multiple_of(part * size, 16), size)
        return remote(
            stage.at[2 * (1 - member) + j, cut, :],
            mixed.at[2 * j + member, place, cut, :],
            swap_send.at[j, part],
            swap_recv.at[j, part],
        )

    def keep(j):
        return pltpu.make_async_copy(stage.at[2 * member + j], mixed.at[2 * j + member, place], keep_sem.at[j])

    def merged_copy(slab):
        return remote(merged.at[slab], merged_in.at[slab], pair_send.at[0, slab], pair_recv.at[0, slab])

    def part_copy(k):
        return remote(part_out.at[k], part_in.at[k], pair_send.at[1, k], pair_recv.at[1, k])

    def round_mixed(group):
        stage[group, :depth, :local] = (value_near[:, group, :] * value_scale[group : group + 1]).astype(jnp.bfloat16)
        stage[group, :depth, local:] = (gate_near[:, group, :] * gate_scale[group : group + 1]).astype(jnp.bfloat16)
        for i in range(2):
            chunk = pool_near[group, i * (cells // 2) : (i + 1) * (cells // 2), :] * pool_scale[group : group + 1]
            stage[group, depth:, i * local : (i + 1) * local] = chunk.astype(jnp.bfloat16)

    def round_up(c):
        wide = hide.shape[3]
        cut = slice(c * wide, (c + 1) * wide)
        hide[c, place] = (up_near[:, cut] * up_scale[:, cut]).astype(jnp.bfloat16)

    def round_down(i):
        part = inner // 4
        at = pl.ds(i * part, part)
        show[place, at, :] = (down_near[at, :] * down_scale[...]).astype(jnp.bfloat16)

    def norm_in(part, parts):
        steps = rows // 16 // parts

        @pl.loop(part * steps, (part + 1) * steps)
        def _(i):
            at = pl.ds(pl.multiple_of(i * 16, 16), 16)
            normed[at, :] = norm_rows(tokens[at, :], mixer_gain[...]).astype(jnp.bfloat16)

    def slab_of(j, q):
        return 2 * j + (member if q == 0 else 1 - member)

    def value_piece(j, q):
        slab = slab_of(j, q)
        weight = mixed[slab, :, :depth, :local].reshape(width, local)
        value = jnp.dot(normed[...], weight, preferred_element_type=jnp.float32)
        floats = value.astype(jnp.bfloat16).astype(jnp.float32)
        position = lax.broadcasted_iota(jnp.int32, floats.shape, 0)
        group = each_group * member + j
        running = floats
        for level in range(groups - each_group + j + 1):
            shifted = pltpu.roll(running, 2**level, 0)
            start = jnp.where(level <= group, 2**level, rows)
            running = running + jnp.where(position >= start, shifted, 0.0)
        window = jnp.int32(2)
        for level in range(groups - 1):
            window = jnp.where(group > level, 2 ** (level + 2), window)
        counts = jnp.minimum(position + 1, window).astype(jnp.float32)
        excess[slab - 2 * j] = (running / counts - floats).astype(jnp.bfloat16)

    def gate_piece(j, q):
        slab = slab_of(j, q)
        gate_weight = mixed[slab, :, :depth, local:].reshape(width, local)
        chunks = [mixed[slab, :, depth:, i * local : (i + 1) * local] for i in range(2)]
        pool = jnp.concatenate(chunks, axis=1).reshape(2 * local, local)

        @pl.loop(0, 2)
        def _(i):
            at = pl.ds(pl.multiple_of(i * half, half), half)
            gate = jnp.dot(normed[at, :], gate_weight, preferred_element_type=jnp.float32)
            pooled = jnp.dot(excess[0, at, :], pool[:local], preferred_element_type=jnp.float32) + jnp.dot(
                excess[1, at, :], pool[local:], preferred_element_type=jnp.float32
            )
            merged[slab, at, :] = (jax.nn.sigmoid(gate) * pooled).astype(jnp.bfloat16)

        merged_copy(slab).start()

    def norm_mid(part, parts):
        if part == 0:
            for slab in range(nm):
                merged_copy(slab).wait_recv()
        steps = rows // 16 // parts

        @pl.loop(part * steps, (part + 1) * steps)
        def _(i):
            at = pl.ds(pl.multiple_of(i * 16, 16), 16)
            held = []
            for slab in range(nm):
                for source, owner in ((merged, member), (merged_in, 1 - member)):
                    cut = pl.ds(pl.multiple_of((nm * owner + slab) * local, local), local)
                    held.append((cut, tokens[at, cut].astype(jnp.float32) + source[slab, at, :].astype(jnp.float32)))
            total = sum(jnp.sum(values * values, axis=-1, keepdims=True) for _, values in held)
            factor = lax.rsqrt(total / width + 1e-06)
            for cut, values in held:
                normed[at, cut] = (values * factor * channel_gain[:, cut]).astype(jnp.bfloat16)

    def up_piece(c, i):
        weight = hide[c, :, :, i * local : (i + 1) * local].reshape(width, local)
        first = c * hide.shape[3] + i * local

        @pl.loop(0, 2)
        def _(b):
            at = pl.ds(pl.multiple_of(b * half, half), half)
            upward = jnp.dot(normed[at, :], weight, preferred_element_type=jnp.float32)
            hidden[at, first : first + local] = jnp.square(jax.nn.relu(upward)).astype(jnp.bfloat16)

    def down_half(k, first):
        at = pl.ds(pl.multiple_of(first, half), half)
        return jnp.dot(hidden[at, :], show[k], preferred_element_type=jnp.float32).astype(jnp.bfloat16)

    def down_step(k):
        part_out[k] = down_half(k, (1 - member) * half)
        part_copy(k).start()
        part_own[k] = down_half(k, member * half)

    def down_at(d, column):
        if d == 0:
            k = g.z * NY + column
            if column is not g.y:
                g.wait_sibling(last, k)
            down_step(k)
            return

        @pl.loop(0, 2)
        def _(way):
            zs = g.z - (2 * way - 1) * d

            @pl.when(g.inside(zs))
            def _():
                k = zs * NY + column
                g.wait_sibling(last, k)
                down_step(k)

    def finish():
        wide = show.shape[2]

        @pl.loop(0, g.nf)
        def _(k):
            part_copy(k).wait_recv()
            cut = pl.ds(pl.multiple_of(k * wide, wide), wide)
            summed = part_own[k].astype(jnp.float32) + part_in[k].astype(jnp.float32)
            out[:, cut] = (middle_of(k) + summed).astype(out.dtype)

    def middle_of(k):
        owner, slab = k // nm, k % nm
        cut = pl.ds(pl.multiple_of(k * local, local), local)
        at = pl.ds(pl.multiple_of(member * half, half), half)
        own = merged[slab, at, :].astype(jnp.float32)
        theirs = merged_in[slab, at, :].astype(jnp.float32)
        return tokens[at, cut].astype(jnp.float32) + jnp.where(owner == member, own, theirs)

    work = []

    def emit(n):
        for _ in range(min(n, len(work))):
            work.pop(0)()

    def add(function, *args):
        work.append(functools.partial(function, *args))

    g.greet()
    for load in loads:
        load.start()
    for load in loads[:3]:
        load.wait()
    for group in range(groups):
        round_mixed(group)
    g.meet()
    swap(0, rep).start()
    g.own(0)
    keep(0).start()
    swap(1, rep).start()
    keep(1).start()
    swap(0, 1 - rep).start()
    swap(1, 1 - rep).start()
    loads[3].wait()
    for i in range(4):
        add(norm_in, i, 4)
    for load in loads[4:]:
        add(load.wait)
    for c in range(nh):
        add(round_up, c)
    for i in range(4):
        add(round_down, i)
    other, pending = 1 - g.y, []
    for phase in range(last + 1):
        g.along(phase, 1)
        g.across(phase, 0)
        if phase + 1 <= last:
            follow = phase + 1
            if follow < nm and follow % 2 == 1:
                swap(follow // 2, rep).wait_recv()
            g.own(follow)
        if phase:
            if phase - 1 < nm and phase % 2 == 0:
                j = (phase - 1) // 2
                keep(j).wait()
                swap(j, 1 - rep).wait_recv()
                g.ready(phase - 2)
                g.ready(phase - 1)
                for q in range(2):
                    add(value_piece, j, q)
                for q in range(2):
                    add(gate_piece, j, q)
            if phase == last - 2:
                for i in range(4):
                    add(norm_mid, i, 4)
            if phase > nm:
                g.ready(phase - 1)
                pending.append(phase - 1 - nm)
            while phase >= last - 2 and pending:
                c = pending.pop(0)
                for i in range(hide.shape[3] // local):
                    add(up_piece, c, i)
        if phase >= 2:
            add(g.drain, phase - 2)
        if phase == last:
            add(down_at, 0, g.y)
            add(down_at, 0, other)
            add(down_at, 1, g.y)
        emit(2)
        for d in range(2, g.nz):
            g.along(phase, d)
            g.across(phase, d - 1)
            if phase == last:
                add(down_at, d, g.y)
                add(down_at, d - 1, other)
            emit(3)
        if phase == last:
            add(g.drain, last - 1)
        g.across(phase, g.nz - 1)
        emit(3)
    emit(len(work))
    down_at(g.nz - 1, other)
    for j in range(2):
        for part in range(2):
            swap(j, part).wait_send()
    for slab in range(nm):
        merged_copy(slab).wait_send()
    g.drain(last)
    finish()

    @pl.loop(0, g.nf)
    def _(k):
        part_copy(k).wait_send()


def run_layer(sizes, vectors, arrays):
    tokens, value, gate, pool, up, down = arrays
    rows, width = tokens.shape
    depth, groups, local = value.shape
    cells = pool.shape[1]
    inner, wide = down.shape
    nf = sizes["fs"]
    vmem = lambda dims, kind=jnp.bfloat16: pltpu.VMEM(tuple(dims), kind)
    halves = (nf, rows // 2, wide)
    count = 12
    return pl.pallas_call(
        functools.partial(layer_kernel, sizes),
        out_shape=jax.ShapeDtypeStruct((rows // 2, width), jnp.bfloat16),
        in_specs=[pl.BlockSpec(memory_space=pltpu.VMEM)] * len(vectors)
        + [pl.BlockSpec(memory_space=pl.ANY)] * len(arrays),
        out_specs=pl.BlockSpec(memory_space=pltpu.VMEM),
        scratch_shapes=[
            vmem((groups, nf, depth + cells // 2, 2 * local)),
            vmem((inner // (2 * local), nf, depth, 2 * local)),
            vmem((nf, inner, wide)),
            vmem((groups, depth + cells // 2, 2 * local)),
            vmem(tokens.shape),
        ]
        + [vmem(array.shape, array.dtype) for array in arrays[1:]]
        + [
            vmem((rows, width)),
            vmem((2, rows, local)),
            vmem((groups, rows, local)),
            vmem((groups, rows, local)),
            vmem((rows, inner)),
            vmem(halves),
            vmem(halves),
            vmem(halves),
            pltpu.SemaphoreType.DMA((4, count, nf)),
            pltpu.SemaphoreType.DMA((2, count, nf)),
            pltpu.SemaphoreType.DMA((len(arrays),)),
            pltpu.SemaphoreType.DMA((2, 2)),
            pltpu.SemaphoreType.DMA((2, 2)),
            pltpu.SemaphoreType.DMA((2,)),
            pltpu.SemaphoreType.DMA((2, nf)),
            pltpu.SemaphoreType.DMA((2, nf)),
        ],
        compiler_params=pltpu.CompilerParams(
            collective_id=0, has_side_effects=True, vmem_limit_bytes=63 * 2**20
        ),
    )(*vectors, *arrays)


def norm_rows(values, gain):
    floats = values.astype(jnp.float32)
    return floats * lax.rsqrt(jnp.mean(floats * floats, axis=-1, keepdims=True) + 1e-06) * gain


def pool_excess(value):
    floats = value.astype(jnp.float32)
    seq_length = floats.shape[1]
    running = floats
    results = []
    for group in range(floats.shape[2]):
        span = 2**group
        shifted = jnp.pad(running, ((0, 0), (span, 0), (0, 0), (0, 0)))[:, :seq_length]
        running = running + shifted
        counts = jnp.minimum(jnp.arange(1, seq_length + 1), 2 * span).astype(jnp.float32)
        results.append(running[:, :, group, :] / counts[None, :, None] - floats[:, :, group, :])
    return jnp.stack(results, axis=2)


def per_device(
    tokens,
    mixer_gain,
    value_weight,
    value_scale,
    gate_weight,
    gate_scale,
    pool_weight,
    pool_scale,
    channel_gain,
    up_weight,
    up_scale,
    down_weight,
    down_scale,
):
    seq_count, seq_length, model_width = tokens.shape
    shares = lax.axis_size("tp")
    member = lax.axis_index("tp")
    kept_rows = seq_length // shares
    row_count = seq_count * seq_length
    group_count, local_width = value_scale.shape
    value_full, gate_full, pool_full = (
        lax.all_gather(value_weight.astype(jnp.bfloat16), "fs", axis=0, tiled=True),
        lax.all_gather(gate_weight.astype(jnp.bfloat16), "fs", axis=0, tiled=True),
        lax.all_gather(pool_weight.astype(jnp.bfloat16), "fs", axis=1, tiled=True),
    )
    down_scales = lax.all_gather(down_scale, "fs", axis=0, tiled=True)
    normed = norm_rows(tokens, mixer_gain).astype(jnp.bfloat16).reshape(row_count, model_width)
    value = jnp.dot(normed, value_full.reshape(model_width, -1), preferred_element_type=jnp.float32)
    value = (
        (value * value_scale.reshape(-1))
        .astype(jnp.bfloat16)
        .reshape(seq_count, seq_length, group_count, local_width)
    )
    gating = jnp.dot(normed, gate_full.reshape(model_width, -1), preferred_element_type=jnp.float32)
    gating = (gating * gate_scale.reshape(-1)).reshape(
        seq_count, seq_length, group_count, local_width
    )
    excess = pool_excess(value).astype(jnp.bfloat16)
    rows_part = pool_full
    pooled = jnp.einsum(
        "slgc,gce->slge",
        lax.all_gather(excess, "tp", axis=3, tiled=True),
        rows_part,
        preferred_element_type=jnp.float32,
    )
    merged = (jax.nn.sigmoid(gating) * (pooled * pool_scale)).astype(jnp.bfloat16)
    merged_own = lax.all_to_all(merged, "tp", split_axis=1, concat_axis=3, tiled=True)
    own_rows = lax.dynamic_slice_in_dim(tokens, member * kept_rows, kept_rows, 1)
    middle = own_rows.reshape(seq_count * kept_rows, model_width).astype(
        jnp.float32
    ) + merged_own.reshape(seq_count * kept_rows, model_width).astype(jnp.float32)
    normed_two = norm_rows(middle, channel_gain).astype(jnp.bfloat16)
    up_full, down_full = (
        lax.all_gather(up_weight.astype(jnp.bfloat16), "fs", axis=0, tiled=True),
        lax.all_gather(down_weight.astype(jnp.bfloat16), "fs", axis=1, tiled=True),
    )
    upward = (
        jnp.dot(
            lax.all_gather(normed_two, "tp", axis=0, tiled=True),
            up_full,
            preferred_element_type=jnp.float32,
        )
        * up_scale
    )
    hidden = jnp.square(jax.nn.relu(upward)).astype(jnp.bfloat16)
    rows_part = hidden
    summed = lax.psum_scatter(
        (jnp.dot(rows_part, down_full, preferred_element_type=jnp.float32) * down_scales).astype(
            jnp.bfloat16
        ),
        "tp",
        scatter_dimension=0,
        tiled=True,
    ).astype(jnp.float32)
    return (middle + summed).astype(jnp.bfloat16).reshape(seq_count, kept_rows, model_width)


def paired_device(
    sizes,
    tokens,
    mixer_gain,
    value_weight,
    value_scale,
    gate_weight,
    gate_scale,
    pool_weight,
    pool_scale,
    channel_gain,
    up_weight,
    up_scale,
    down_weight,
    down_scale,
):
    row = lambda vector: vector.reshape(1, -1)
    out = run_layer(
        sizes,
        (row(mixer_gain), value_scale, gate_scale, pool_scale, row(channel_gain), row(up_scale), row(down_scale)),
        (tokens[0], value_weight, gate_weight, pool_weight, up_weight, down_weight),
    )
    return out[None]


def solution(mesh):
    sizes = dict(mesh.shape)
    paired = sizes["rep"] == 2 and sizes["tp"] == 2 and sizes["fs"] == 8

    def body(tokens, *rest):
        value_scale, down_scale = rest[2], rest[-1]
        square = value_scale.shape[1] == down_scale.shape[0] == rest[1].shape[0]
        if paired and tokens.shape[0] == 1 and square and value_scale.shape[0] == 4:
            return paired_device(sizes, tokens, *rest)
        return per_device(tokens, *rest)

    return jax.shard_map(
        body,
        mesh=mesh,
        in_specs=(
            P(("rep", "fs"), None, None),
            P(),
            P("fs", None, "tp"),
            P(None, "tp"),
            P("fs", None, "tp"),
            P(None, "tp"),
            P(None, "fs", "tp"),
            P(None, "tp"),
            P(),
            P("fs", "tp"),
            P("tp"),
            P("tp", "fs"),
            P("fs"),
        ),
        out_specs=P(("rep", "fs"), "tp", None),
        check_vma=False,
    )
```

```python
import functools

import jax
import jax.numpy as jnp
from jax import lax
from jax.experimental import pallas as pl
from jax.experimental.pallas import tpu as pltpu
from jax.sharding import PartitionSpec as P

NY = 2
ACROSS, SIBLING = 2, 3


class Gather:
    def __init__(self, sizes, bufs, sems):
        self.nf = sizes["fs"]
        self.nz = self.nf // NY
        self.rep, self.place, self.tp = lax.axis_index("rep"), lax.axis_index("fs"), lax.axis_index("tp")
        self.z, self.y = self.place // NY, self.place % NY
        self.mixed, self.hide, self.show, self.stage = bufs
        self.send_sem, self.recv_sem = sems
        self.nm, self.nh = self.mixed.shape[0], self.hide.shape[0]
        self.subs = 4
        self.count = self.nm + self.nh + self.subs

    def device(self, way):
        rep, place = self.rep, self.place
        if isinstance(way, int) and way == ACROSS:
            place = self.z * NY + 1 - self.y
        elif isinstance(way, int) and way == SIBLING:
            rep = 1 - rep
        else:
            place = place + NY * (2 * way - 1)
        return {"rep": rep, "fs": place, "tp": self.tp}

    def partner(self):
        return {"rep": self.rep, "fs": self.place, "tp": 1 - self.tp}

    def half_of(self, p):
        j, q = p // 2, p % 2
        return 2 * j + (self.tp if q == 0 else 1 - self.tp)

    def piece(self, p, k, half):
        if isinstance(p, int) and p < self.nm:
            part = self.mixed.shape[2] // 2
            return self.mixed.at[self.half_of(p), k, pl.ds(pl.multiple_of(half * part, 16), part), :]
        if isinstance(p, int) and p < self.nm + self.nh:
            part = self.hide.shape[2] // 2
            return self.hide.at[p - self.nm, k, pl.ds(pl.multiple_of(half * part, 16), part), :]
        part = self.show.shape[1] // (2 * self.subs)
        sub = p - self.nm - self.nh
        return self.show.at[k, pl.ds(pl.multiple_of((2 * sub + half) * part, 16), part), :]

    def copy(self, p, k, way, half=None, src=None):
        half = self.rep if half is None else half
        sibling = isinstance(way, int) and way == SIBLING
        return pltpu.make_async_remote_copy(
            src_ref=self.piece(p, k, half) if src is None else src,
            dst_ref=self.piece(p, k, half),
            send_sem=self.send_sem.at[way, p, k],
            recv_sem=self.recv_sem.at[1 if sibling else 0, p, k],
            device_id=self.device(way),
            device_id_type=pl.DeviceIdType.MESH,
        )

    def inside(self, z):
        return (z >= 0) & (z < self.nz)

    def wide(self, p, zs):
        return ((zs == 0) | (zs == self.nz - 1)) & (self.rep == p % 2)

    def greet(self):
        sem = pltpu.get_barrier_semaphore()

        def signal(device):
            pl.semaphore_signal(sem, inc=1, device_id=device, device_id_type=pl.DeviceIdType.MESH)

        signal(self.device(ACROSS))
        signal(self.device(SIBLING))
        signal(self.partner())
        pl.when(self.z > 0)(lambda: signal(self.device(0)))
        pl.when(self.z < self.nz - 1)(lambda: signal(self.device(1)))

    def meet(self):
        ends = (self.z > 0).astype(jnp.int32) + (self.z < self.nz - 1).astype(jnp.int32)
        pl.semaphore_wait(pltpu.get_barrier_semaphore(), 3 + ends)

    def each(self, phase, body):
        first = 2 * phase
        if first < self.nm + self.nh:
            for p in (first, first + 1):
                body(p)
        else:
            pl.loop(0, self.subs)(lambda sub: body(first + sub))

    def source(self, p):
        if not (isinstance(p, int) and p < self.nm and p % 2 == 0):
            return None
        part = self.stage.shape[1] // 2
        rows = pl.ds(pl.multiple_of(self.rep * part, 16), part)
        return self.stage.at[2 * self.tp + p // 2, rows, :]

    def own_in(self, *pieces):
        for p in pieces:
            src = self.source(p)
            way = (self.z == 0).astype(jnp.int32)
            end = (self.z == 0) | (self.z == self.nz - 1)
            pl.when(end)(lambda: self.copy(p, self.place, way, src=src).start())

    def own_out(self, *pieces):
        for p in pieces:
            src = self.source(p)

            @pl.when((self.z > 0) & (self.z < self.nz - 1))
            def _():
                for way in range(2):
                    self.copy(p, self.place, way, src=src).start()

            self.copy(p, self.place, ACROSS, src=src).start()

    def own(self, *pieces):
        self.own_in(*pieces)
        self.own_out(*pieces)

    def along(self, phase, d):
        @pl.loop(0, 2)
        def _(way):
            step = 2 * way - 1
            zs = self.z - step * d

            @pl.when(self.inside(zs))
            def _():
                k = zs * NY + self.y

                def body(p):
                    self.copy(p, k, ACROSS).wait_recv()
                    pl.when(self.inside(self.z + step))(lambda: self.copy(p, k, way).start())
                    pl.when(jnp.logical_not(self.wide(p, zs)))(lambda: self.copy(p, k, ACROSS).start())
                    self.copy(p, k, SIBLING).start()

                self.each(phase, body)

    def facing(self, phase):
        k = self.z * NY + 1 - self.y
        way = (self.z == 0).astype(jnp.int32)

        def body(p):
            self.copy(p, k, ACROSS).wait_recv()
            pl.when(self.wide(p, self.z))(lambda: self.copy(p, k, way).start())
            self.copy(p, k, SIBLING).start()

        self.each(phase, body)

    def across(self, phase, d, wide):
        @pl.loop(0, 2)
        def _(way):
            step = 2 * way - 1
            zs = self.z - step * d
            k = zs * NY + 1 - self.y

            def body(p):
                @pl.when(self.wide(p, zs) if wide else jnp.logical_not(self.wide(p, zs)))
                def _():
                    self.copy(p, k, ACROSS).wait_recv()
                    if wide:
                        pl.when(self.inside(self.z + step))(lambda: self.copy(p, k, way).start())
                    self.copy(p, k, SIBLING).start()

            pl.when(self.inside(zs))(lambda: self.each(phase, body))

    def wait_sibling(self, phase, k):
        self.each(phase, lambda p: self.copy(p, k, SIBLING, half=1 - self.rep).wait_recv())

    def ready(self, p):
        @pl.loop(0, self.nf)
        def _(k):
            pl.when(k != self.place)(lambda: self.copy(p, k, SIBLING, half=1 - self.rep).wait_recv())

    def drain(self, phase):
        def body(p):
            src = self.source(p)

            @pl.loop(0, self.nf)
            def _(k):
                zs, mine = k // NY, k % NY == self.y
                wide = self.wide(p, zs)
                here = zs == self.z

                @pl.loop(0, 2)
                def _(way):
                    step = 2 * way - 1
                    away = here | (step * (self.z - zs) > 0)
                    sent = self.inside(self.z + step) & away & (mine | wide)
                    pl.when(sent)(lambda: self.copy(p, k, way).wait_send())

                pl.when(mine & (here | jnp.logical_not(wide)))(lambda: self.copy(p, k, ACROSS).wait_send())
                pl.when(k != self.place)(lambda: self.copy(p, k, SIBLING).wait_send())

        self.each(phase, body)


def layer_kernel(sizes, *refs):
    mixer_gain, value_scale, gate_scale, pool_scale, channel_gain, up_scale, down_scale = refs[:7]
    tokens_far, value_far, gate_far, pool_far, up_far, down_far, out = refs[7:14]
    mixed, hide, show, stage = refs[14:18]
    tokens, value_near, gate_near, pool_near, up_near, down_near = refs[18:24]
    normed, excess, merged, merged_in, hidden, part_out, part_own, part_in = refs[24:32]
    send_sem, recv_sem, load_sem, swap_send, swap_recv, keep_sem, pair_send, pair_recv = refs[32:]
    g = Gather(sizes, (mixed, hide, show, stage), (send_sem, recv_sem))
    rows, width = tokens.shape
    groups, cells, local = pool_near.shape
    depth = value_near.shape[0]
    half = rows // 2
    inner = hidden.shape[1]
    member, rep, place = g.tp, g.rep, g.place
    nm, nh = g.nm, g.nh
    last = nm + nh
    each_group = nm // 2

    loads = [
        pltpu.make_async_copy(far, near, load_sem.at[i])
        for i, (far, near) in enumerate(
            (
                (value_far, value_near),
                (gate_far, gate_near),
                (pool_far, pool_near),
                (tokens_far, tokens),
                (up_far, up_near),
                (down_far, down_near),
            )
        )
    ]

    def remote(source, target, send, recv):
        return pltpu.make_async_remote_copy(
            src_ref=source,
            dst_ref=target,
            send_sem=send,
            recv_sem=recv,
            device_id=g.partner(),
            device_id_type=pl.DeviceIdType.MESH,
        )

    def swap(j, part):
        size = stage.shape[1] // 2
        cut = pl.ds(pl.multiple_of(part * size, 16), size)
        return remote(
            stage.at[2 * (1 - member) + j, cut, :],
            mixed.at[2 * j + member, place, cut, :],
            swap_send.at[j, part],
            swap_recv.at[j, part],
        )

    def keep(j):
        return pltpu.make_async_copy(stage.at[2 * member + j], mixed.at[2 * j + member, place], keep_sem.at[j])

    def merged_copy(slab):
        return remote(merged.at[slab], merged_in.at[slab], pair_send.at[0, slab], pair_recv.at[0, slab])

    def part_copy(k):
        return remote(part_out.at[k], part_in.at[k], pair_send.at[1, k], pair_recv.at[1, k])

    def round_mixed(group):
        stage[group, :depth, :local] = (value_near[:, group, :] * value_scale[group : group + 1]).astype(jnp.bfloat16)
        stage[group, :depth, local:] = (gate_near[:, group, :] * gate_scale[group : group + 1]).astype(jnp.bfloat16)
        for i in range(2):
            chunk = pool_near[group, i * (cells // 2) : (i + 1) * (cells // 2), :] * pool_scale[group : group + 1]
            stage[group, depth:, i * local : (i + 1) * local] = chunk.astype(jnp.bfloat16)

    def round_up(c):
        wide = hide.shape[3]
        cut = slice(c * wide, (c + 1) * wide)
        hide[c, place] = (up_near[:, cut] * up_scale[:, cut]).astype(jnp.bfloat16)

    def round_down(i):
        part = inner // 4
        at = pl.ds(i * part, part)
        show[place, at, :] = (down_near[at, :] * down_scale[...]).astype(jnp.bfloat16)

    def norm_in(part, parts):
        steps = rows // 16 // parts

        @pl.loop(part * steps, (part + 1) * steps)
        def _(i):
            at = pl.ds(pl.multiple_of(i * 16, 16), 16)
            normed[at, :] = norm_rows(tokens[at, :], mixer_gain[...]).astype(jnp.bfloat16)

    def slab_of(j, q):
        return 2 * j + (member if q == 0 else 1 - member)

    def value_piece(j, q):
        slab = slab_of(j, q)
        weight = mixed[slab, :, :depth, :local].reshape(width, local)
        value = jnp.dot(normed[...], weight, preferred_element_type=jnp.float32)
        floats = value.astype(jnp.bfloat16).astype(jnp.float32)
        position = lax.broadcasted_iota(jnp.int32, floats.shape, 0)
        group = each_group * member + j
        running = floats
        for level in range(groups - each_group + j + 1):
            shifted = pltpu.roll(running, 2**level, 0)
            start = jnp.where(level <= group, 2**level, rows)
            running = running + jnp.where(position >= start, shifted, 0.0)
        window = jnp.int32(2)
        for level in range(groups - 1):
            window = jnp.where(group > level, 2 ** (level + 2), window)
        counts = jnp.minimum(position + 1, window).astype(jnp.float32)
        excess[slab - 2 * j] = (running / counts - floats).astype(jnp.bfloat16)

    def gate_piece(j, q):
        slab = slab_of(j, q)
        gate_weight = mixed[slab, :, :depth, local:].reshape(width, local)
        chunks = [mixed[slab, :, depth:, i * local : (i + 1) * local] for i in range(2)]
        pool = jnp.concatenate(chunks, axis=1).reshape(2 * local, local)

        @pl.loop(0, 2)
        def _(i):
            at = pl.ds(pl.multiple_of(i * half, half), half)
            gate = jnp.dot(normed[at, :], gate_weight, preferred_element_type=jnp.float32)
            pooled = jnp.dot(excess[0, at, :], pool[:local], preferred_element_type=jnp.float32) + jnp.dot(
                excess[1, at, :], pool[local:], preferred_element_type=jnp.float32
            )
            merged[slab, at, :] = (jax.nn.sigmoid(gate) * pooled).astype(jnp.bfloat16)

        merged_copy(slab).start()

    def norm_mid(part, parts):
        if part == 0:
            for slab in range(nm):
                merged_copy(slab).wait_recv()
        steps = rows // 16 // parts

        @pl.loop(part * steps, (part + 1) * steps)
        def _(i):
            at = pl.ds(pl.multiple_of(i * 16, 16), 16)
            held = []
            for slab in range(nm):
                for source, owner in ((merged, member), (merged_in, 1 - member)):
                    cut = pl.ds(pl.multiple_of((nm * owner + slab) * local, local), local)
                    held.append((cut, tokens[at, cut].astype(jnp.float32) + source[slab, at, :].astype(jnp.float32)))
            total = sum(jnp.sum(values * values, axis=-1, keepdims=True) for _, values in held)
            factor = lax.rsqrt(total / width + 1e-06)
            for cut, values in held:
                normed[at, cut] = (values * factor * channel_gain[:, cut]).astype(jnp.bfloat16)

    def up_piece(c, i):
        weight = hide[c, :, :, i * local : (i + 1) * local].reshape(width, local)
        first = c * hide.shape[3] + i * local

        @pl.loop(0, 2)
        def _(b):
            at = pl.ds(pl.multiple_of(b * half, half), half)
            upward = jnp.dot(normed[at, :], weight, preferred_element_type=jnp.float32)
            hidden[at, first : first + local] = jnp.square(jax.nn.relu(upward)).astype(jnp.bfloat16)

    def down_half(k, first):
        at = pl.ds(pl.multiple_of(first, half), half)
        return jnp.dot(hidden[at, :], show[k], preferred_element_type=jnp.float32).astype(jnp.bfloat16)

    def down_step(k):
        part_out[k] = down_half(k, (1 - member) * half)
        part_copy(k).start()
        part_own[k] = down_half(k, member * half)

    def down_at(d, column):
        if d == 0:
            k = g.z * NY + column
            if column is not g.y:
                g.wait_sibling(last // 2, k)
            down_step(k)
            return

        @pl.loop(0, 2)
        def _(way):
            zs = g.z - (2 * way - 1) * d

            @pl.when(g.inside(zs))
            def _():
                k = zs * NY + column
                g.wait_sibling(last // 2, k)
                down_step(k)

    def finish(k):
        wide = show.shape[2]
        part_copy(k).wait_recv()
        cut = pl.ds(pl.multiple_of(k * wide, wide), wide)
        summed = part_own[k].astype(jnp.float32) + part_in[k].astype(jnp.float32)
        out[:, cut] = (middle_of(k) + summed).astype(out.dtype)

    def finish_at(d, column):
        @pl.loop(0, 1 if d == 0 else 2)
        def _(way):
            zs = g.z - (2 * way - 1) * d
            pl.when(g.inside(zs))(lambda: finish(zs * NY + column))

    def middle_of(k):
        owner, slab = k // nm, k % nm
        cut = pl.ds(pl.multiple_of(k * local, local), local)
        at = pl.ds(pl.multiple_of(member * half, half), half)
        own = merged[slab, at, :].astype(jnp.float32)
        theirs = merged_in[slab, at, :].astype(jnp.float32)
        return tokens[at, cut].astype(jnp.float32) + jnp.where(owner == member, own, theirs)

    work = []

    def emit(n):
        for _ in range(min(n, len(work))):
            work.pop(0)()

    def add(function, *args):
        work.append(functools.partial(function, *args))

    g.greet()
    for load in loads:
        load.start()
    for load in loads[:3]:
        load.wait()
    for group in range(groups):
        round_mixed(group)
    g.meet()
    swap(0, rep).start()
    g.own(0)
    g.own(2)
    for j in range(each_group):
        keep(j).start()
    swap(0, rep).wait_recv()
    g.own(1)
    swap(1, rep).start()
    for j in range(each_group):
        swap(j, 1 - rep).start()

    def mix(j):
        keep(j).wait()
        swap(j, 1 - rep).wait_recv()
        for q in range(2):
            g.ready(2 * j + q)
            add(value_piece, j, q)
        for q in range(2):
            add(gate_piece, j, q)

    def lift(c):
        g.ready(nm + c)
        for i in range(hide.shape[3] // local):
            add(up_piece, c, i)

    def load_up():
        loads[4].wait()
        for c in range(nh):
            round_up(c)

    def load_down():
        loads[5].wait()
        for i in range(4):
            round_down(i)

    show_pieces = tuple(range(last, g.count))
    inward = ((4, 5), (6, 7), show_pieces, ())
    outward = ((3,), (4, 5), (6, 7), show_pieces)

    def next_own(phase):
        g.own_out(*outward[phase])
        g.own_in(*inward[phase])

    other, show_phase = 1 - g.y, last // 2
    add(load_up)
    add(loads[3].wait)
    for i in range(4):
        add(norm_in, i, 4)
    add(load_down)
    emits = ((3, 1, 1, 1, 1, 0, 0, 2), (1, 1, 0, 0, 0, 0, 0, 2), (1, 1, 1, 0, 0, 0, 0, 0), (0, 1, 1, 3, 2, 1, 0, 0))
    far = g.nz - 1
    for phase in range(show_phase):
        counts = emits[phase]
        if phase == show_phase - 1:
            for i in range(4):
                add(norm_mid, i, 4)
        g.along(phase, 1)
        if phase == 0:
            swap(1, rep).wait_recv()
            g.own_in(3)
        emit(counts[0])
        g.facing(phase)
        emit(counts[1])
        g.along(phase, 2)
        g.across(phase, 1, True)
        emit(counts[2])
        g.along(phase, 3)
        g.across(phase, 2, True)
        next_own(phase)
        if phase == show_phase - 1:
            for c in range(nh - 2):
                lift(c)
        emit(counts[3])
        g.across(phase, 1, False)
        emit(counts[4])
        g.across(phase, 2, False)
        emit(counts[5])
        g.across(phase, 3, True)
        emit(counts[6])
        g.across(phase, 3, False)
        if phase < each_group:
            mix(phase)
        emit(counts[7])
        if phase == 1:
            add(g.drain, 0)
        elif phase == 2:
            g.drain(1)
    lift(nh - 2)
    lift(nh - 1)
    add(down_at, 0, g.y)
    emit(len(work))
    g.along(show_phase, 1)
    down_at(1, g.y)
    g.facing(show_phase)
    down_at(0, other)
    g.drain(2)
    g.along(show_phase, 2)
    g.across(show_phase, 1, True)
    down_at(2, g.y)
    g.drain(3)
    g.across(show_phase, 1, False)
    down_at(1, other)
    g.along(show_phase, 3)
    g.across(show_phase, 2, True)
    finish_at(0, g.y)
    down_at(3, g.y)
    g.across(show_phase, 2, False)
    down_at(2, other)
    finish_at(1, g.y)
    finish_at(0, other)
    g.across(show_phase, 3, True)
    g.across(show_phase, 3, False)
    down_at(3, other)
    finish_at(2, g.y)
    finish_at(1, other)
    for j in range(each_group):
        for part in range(2):
            swap(j, part).wait_send()
    for slab in range(nm):
        merged_copy(slab).wait_send()
    g.drain(show_phase)
    finish_at(far, g.y)
    finish_at(2, other)
    finish_at(far, other)

    @pl.loop(0, g.nf)
    def _(k):
        part_copy(k).wait_send()


def run_layer(sizes, vectors, arrays):
    tokens, value, gate, pool, up, down = arrays
    rows, width = tokens.shape
    depth, groups, local = value.shape
    cells = pool.shape[1]
    inner, wide = down.shape
    nf = sizes["fs"]
    vmem = lambda dims, kind=jnp.bfloat16: pltpu.VMEM(tuple(dims), kind)
    halves = (nf, rows // 2, wide)
    count = 12
    sems = [
        pltpu.SemaphoreType.DMA((4, count, nf)),
        pltpu.SemaphoreType.DMA((2, count, nf)),
        pltpu.SemaphoreType.DMA((len(arrays),)),
        pltpu.SemaphoreType.DMA((2, 2)),
        pltpu.SemaphoreType.DMA((2, 2)),
        pltpu.SemaphoreType.DMA((2,)),
        pltpu.SemaphoreType.DMA((2, nf)),
        pltpu.SemaphoreType.DMA((2, nf)),
    ]
    kernel = lambda *refs: pl.run_scoped(functools.partial(layer_kernel, sizes, *refs), *sems)
    return pl.pallas_call(
        kernel,
        out_shape=jax.ShapeDtypeStruct((rows // 2, width), jnp.bfloat16),
        in_specs=[pl.BlockSpec(memory_space=pltpu.VMEM)] * len(vectors)
        + [pl.BlockSpec(memory_space=pl.ANY)] * len(arrays),
        out_specs=pl.BlockSpec(memory_space=pltpu.VMEM),
        scratch_shapes=[
            vmem((groups, nf, depth + cells // 2, 2 * local)),
            vmem((inner // (2 * local), nf, depth, 2 * local)),
            vmem((nf, inner, wide)),
            vmem((groups, depth + cells // 2, 2 * local)),
            vmem(tokens.shape),
        ]
        + [vmem(array.shape, array.dtype) for array in arrays[1:]]
        + [
            vmem((rows, width)),
            vmem((2, rows, local)),
            vmem((groups, rows, local)),
            vmem((groups, rows, local)),
            vmem((rows, inner)),
            vmem(halves),
            vmem(halves),
            vmem(halves),
        ],
        compiler_params=pltpu.CompilerParams(
            collective_id=0, has_side_effects=True, vmem_limit_bytes=63 * 2**20
        ),
    )(*vectors, *arrays)


def norm_rows(values, gain):
    floats = values.astype(jnp.float32)
    return floats * lax.rsqrt(jnp.mean(floats * floats, axis=-1, keepdims=True) + 1e-06) * gain


def pool_excess(value):
    floats = value.astype(jnp.float32)
    seq_length = floats.shape[1]
    running = floats
    results = []
    for group in range(floats.shape[2]):
        span = 2**group
        shifted = jnp.pad(running, ((0, 0), (span, 0), (0, 0), (0, 0)))[:, :seq_length]
        running = running + shifted
        counts = jnp.minimum(jnp.arange(1, seq_length + 1), 2 * span).astype(jnp.float32)
        results.append(running[:, :, group, :] / counts[None, :, None] - floats[:, :, group, :])
    return jnp.stack(results, axis=2)


def per_device(
    tokens,
    mixer_gain,
    value_weight,
    value_scale,
    gate_weight,
    gate_scale,
    pool_weight,
    pool_scale,
    channel_gain,
    up_weight,
    up_scale,
    down_weight,
    down_scale,
):
    seq_count, seq_length, model_width = tokens.shape
    shares = lax.axis_size("tp")
    member = lax.axis_index("tp")
    kept_rows = seq_length // shares
    row_count = seq_count * seq_length
    group_count, local_width = value_scale.shape
    value_full, gate_full, pool_full = (
        lax.all_gather(value_weight.astype(jnp.bfloat16), "fs", axis=0, tiled=True),
        lax.all_gather(gate_weight.astype(jnp.bfloat16), "fs", axis=0, tiled=True),
        lax.all_gather(pool_weight.astype(jnp.bfloat16), "fs", axis=1, tiled=True),
    )
    down_scales = lax.all_gather(down_scale, "fs", axis=0, tiled=True)
    normed = norm_rows(tokens, mixer_gain).astype(jnp.bfloat16).reshape(row_count, model_width)
    value = jnp.dot(normed, value_full.reshape(model_width, -1), preferred_element_type=jnp.float32)
    value = (
        (value * value_scale.reshape(-1))
        .astype(jnp.bfloat16)
        .reshape(seq_count, seq_length, group_count, local_width)
    )
    gating = jnp.dot(normed, gate_full.reshape(model_width, -1), preferred_element_type=jnp.float32)
    gating = (gating * gate_scale.reshape(-1)).reshape(
        seq_count, seq_length, group_count, local_width
    )
    excess = pool_excess(value).astype(jnp.bfloat16)
    rows_part = pool_full
    pooled = jnp.einsum(
        "slgc,gce->slge",
        lax.all_gather(excess, "tp", axis=3, tiled=True),
        rows_part,
        preferred_element_type=jnp.float32,
    )
    merged = (jax.nn.sigmoid(gating) * (pooled * pool_scale)).astype(jnp.bfloat16)
    merged_own = lax.all_to_all(merged, "tp", split_axis=1, concat_axis=3, tiled=True)
    own_rows = lax.dynamic_slice_in_dim(tokens, member * kept_rows, kept_rows, 1)
    middle = own_rows.reshape(seq_count * kept_rows, model_width).astype(
        jnp.float32
    ) + merged_own.reshape(seq_count * kept_rows, model_width).astype(jnp.float32)
    normed_two = norm_rows(middle, channel_gain).astype(jnp.bfloat16)
    up_full, down_full = (
        lax.all_gather(up_weight.astype(jnp.bfloat16), "fs", axis=0, tiled=True),
        lax.all_gather(down_weight.astype(jnp.bfloat16), "fs", axis=1, tiled=True),
    )
    upward = (
        jnp.dot(
            lax.all_gather(normed_two, "tp", axis=0, tiled=True),
            up_full,
            preferred_element_type=jnp.float32,
        )
        * up_scale
    )
    hidden = jnp.square(jax.nn.relu(upward)).astype(jnp.bfloat16)
    rows_part = hidden
    summed = lax.psum_scatter(
        (jnp.dot(rows_part, down_full, preferred_element_type=jnp.float32) * down_scales).astype(
            jnp.bfloat16
        ),
        "tp",
        scatter_dimension=0,
        tiled=True,
    ).astype(jnp.float32)
    return (middle + summed).astype(jnp.bfloat16).reshape(seq_count, kept_rows, model_width)


def paired_device(
    sizes,
    tokens,
    mixer_gain,
    value_weight,
    value_scale,
    gate_weight,
    gate_scale,
    pool_weight,
    pool_scale,
    channel_gain,
    up_weight,
    up_scale,
    down_weight,
    down_scale,
):
    row = lambda vector: vector.reshape(1, -1)
    out = run_layer(
        sizes,
        (row(mixer_gain), value_scale, gate_scale, pool_scale, row(channel_gain), row(up_scale), row(down_scale)),
        (tokens[0], value_weight, gate_weight, pool_weight, up_weight, down_weight),
    )
    return out[None]


def solution(mesh):
    sizes = dict(mesh.shape)
    paired = sizes["rep"] == 2 and sizes["tp"] == 2 and sizes["fs"] == 8

    def body(tokens, *rest):
        value_scale, down_scale = rest[2], rest[-1]
        square = value_scale.shape[1] == down_scale.shape[0] == rest[1].shape[0]
        if paired and tokens.shape[0] == 1 and square and value_scale.shape[0] == 4:
            return paired_device(sizes, tokens, *rest)
        return per_device(tokens, *rest)

    return jax.shard_map(
        body,
        mesh=mesh,
        in_specs=(
            P(("rep", "fs"), None, None),
            P(),
            P("fs", None, "tp"),
            P(None, "tp"),
            P("fs", None, "tp"),
            P(None, "tp"),
            P(None, "fs", "tp"),
            P(None, "tp"),
            P(),
            P("fs", "tp"),
            P("tp"),
            P("tp", "fs"),
            P("fs"),
        ),
        out_specs=P(("rep", "fs"), "tp", None),
        check_vma=False,
    )
```

```python
import functools

import jax
import jax.numpy as jnp
from jax import lax
from jax.experimental import pallas as pl
from jax.experimental.pallas import tpu as pltpu
from jax.sharding import PartitionSpec as P

NY = 2
ACROSS, SIBLING = 2, 3


class Gather:
    def __init__(self, sizes, bufs, sems):
        self.nf = sizes["fs"]
        self.nz = self.nf // NY
        self.rep, self.place, self.tp = lax.axis_index("rep"), lax.axis_index("fs"), lax.axis_index("tp")
        self.z, self.y = self.place // NY, self.place % NY
        self.mixed, self.hide, self.show, self.stage = bufs
        self.send_sem, self.recv_sem = sems
        self.nm, self.nh = self.mixed.shape[0], self.hide.shape[0]
        self.subs = 4
        self.count = self.nm + self.nh + self.subs

    def device(self, way):
        rep, place = self.rep, self.place
        if isinstance(way, int) and way == ACROSS:
            place = self.z * NY + 1 - self.y
        elif isinstance(way, int) and way == SIBLING:
            rep = 1 - rep
        else:
            place = place + NY * (2 * way - 1)
        return {"rep": rep, "fs": place, "tp": self.tp}

    def partner(self):
        return {"rep": self.rep, "fs": self.place, "tp": 1 - self.tp}

    def half_of(self, p):
        j, q = p // 2, p % 2
        return 2 * j + (self.tp if q == 0 else 1 - self.tp)

    def piece(self, p, k, half):
        if p < self.nm:
            part = self.mixed.shape[2] // 2
            return self.mixed.at[self.half_of(p), k, pl.ds(pl.multiple_of(half * part, 16), part), :]
        if p < self.nm + self.nh:
            part = self.hide.shape[2] // 2
            return self.hide.at[p - self.nm, k, pl.ds(pl.multiple_of(half * part, 16), part), :]
        part = self.show.shape[2] // 4
        side, deep = (p - self.nm - self.nh) // 2, p % 2
        return self.show.at[k, side, pl.ds(pl.multiple_of((2 * deep + half) * part, 16), part), :]

    def copy(self, p, k, way, half=None, src=None):
        half = self.rep if half is None else half
        sibling = isinstance(way, int) and way == SIBLING
        return pltpu.make_async_remote_copy(
            src_ref=self.piece(p, k, half) if src is None else src,
            dst_ref=self.piece(p, k, half),
            send_sem=self.send_sem.at[way, p, k],
            recv_sem=self.recv_sem.at[1 if sibling else 0, p, k],
            device_id=self.device(way),
            device_id_type=pl.DeviceIdType.MESH,
        )

    def inside(self, z):
        return (z >= 0) & (z < self.nz)

    def wide(self, p, zs):
        return ((zs == 0) | (zs == self.nz - 1)) & (self.rep == p % 2)

    def greet(self):
        sem = pltpu.get_barrier_semaphore()

        def signal(device):
            pl.semaphore_signal(sem, inc=1, device_id=device, device_id_type=pl.DeviceIdType.MESH)

        signal(self.device(ACROSS))
        signal(self.device(SIBLING))
        signal(self.partner())
        pl.when(self.z > 0)(lambda: signal(self.device(0)))
        pl.when(self.z < self.nz - 1)(lambda: signal(self.device(1)))

    def meet(self):
        ends = (self.z > 0).astype(jnp.int32) + (self.z < self.nz - 1).astype(jnp.int32)
        pl.semaphore_wait(pltpu.get_barrier_semaphore(), 3 + ends)

    def each(self, phase, body):
        for p in (2 * phase, 2 * phase + 1):
            body(p)

    def source(self, p):
        if p >= self.nm or p % 2:
            return None
        part = self.stage.shape[1] // 2
        rows = pl.ds(pl.multiple_of(self.rep * part, 16), part)
        return self.stage.at[2 * self.tp + p // 2, rows, :]

    def own_in(self, *pieces):
        for p in pieces:
            src = self.source(p)
            way = (self.z == 0).astype(jnp.int32)
            end = (self.z == 0) | (self.z == self.nz - 1)
            pl.when(end)(lambda: self.copy(p, self.place, way, src=src).start())

    def own_out(self, *pieces):
        for p in pieces:
            src = self.source(p)

            @pl.when((self.z > 0) & (self.z < self.nz - 1))
            def _():
                for way in range(2):
                    self.copy(p, self.place, way, src=src).start()

            self.copy(p, self.place, ACROSS, src=src).start()

    def own(self, *pieces):
        self.own_in(*pieces)
        self.own_out(*pieces)

    def along(self, phase, d):
        @pl.loop(0, 2)
        def _(way):
            step = 2 * way - 1
            zs = self.z - step * d

            @pl.when(self.inside(zs))
            def _():
                k = zs * NY + self.y

                def body(p):
                    self.copy(p, k, ACROSS).wait_recv()
                    pl.when(self.inside(self.z + step))(lambda: self.copy(p, k, way).start())
                    pl.when(jnp.logical_not(self.wide(p, zs)))(lambda: self.copy(p, k, ACROSS).start())
                    self.copy(p, k, SIBLING).start()

                self.each(phase, body)

    def facing(self, phase):
        k = self.z * NY + 1 - self.y
        way = (self.z == 0).astype(jnp.int32)

        def body(p):
            self.copy(p, k, ACROSS).wait_recv()
            pl.when(self.wide(p, self.z))(lambda: self.copy(p, k, way).start())
            self.copy(p, k, SIBLING).start()

        self.each(phase, body)

    def across(self, phase, d, wide):
        @pl.loop(0, 2)
        def _(way):
            step = 2 * way - 1
            zs = self.z - step * d
            k = zs * NY + 1 - self.y

            def body(p):
                @pl.when(self.wide(p, zs) if wide else jnp.logical_not(self.wide(p, zs)))
                def _():
                    self.copy(p, k, ACROSS).wait_recv()
                    if wide:
                        pl.when(self.inside(self.z + step))(lambda: self.copy(p, k, way).start())
                    self.copy(p, k, SIBLING).start()

            pl.when(self.inside(zs))(lambda: self.each(phase, body))

    def wait_sibling(self, phase, k):
        self.each(phase, lambda p: self.copy(p, k, SIBLING, half=1 - self.rep).wait_recv())

    def ready(self, p):
        @pl.loop(0, self.nf)
        def _(k):
            pl.when(k != self.place)(lambda: self.copy(p, k, SIBLING, half=1 - self.rep).wait_recv())

    def drain(self, phase):
        def body(p):
            src = self.source(p)

            @pl.loop(0, self.nf)
            def _(k):
                zs, mine = k // NY, k % NY == self.y
                wide = self.wide(p, zs)
                here = zs == self.z

                @pl.loop(0, 2)
                def _(way):
                    step = 2 * way - 1
                    away = here | (step * (self.z - zs) > 0)
                    sent = self.inside(self.z + step) & away & (mine | wide)
                    pl.when(sent)(lambda: self.copy(p, k, way).wait_send())

                pl.when(mine & (here | jnp.logical_not(wide)))(lambda: self.copy(p, k, ACROSS).wait_send())
                pl.when(k != self.place)(lambda: self.copy(p, k, SIBLING).wait_send())

        self.each(phase, body)


def layer_kernel(sizes, *refs):
    mixer_gain, value_scale, gate_scale, pool_scale, channel_gain, up_scale, down_scale = refs[:7]
    tokens_far, value_far, gate_far, pool_far, up_far, down_far, out = refs[7:14]
    mixed, hide, show, stage = refs[14:18]
    tokens, value_near, gate_near, pool_near, up_near, down_near = refs[18:24]
    normed, excess, merged, merged_in, hidden, parts, part_in = refs[24:31]
    send_sem, recv_sem, load_sem, swap_send, swap_recv, keep_sem, pair_send, pair_recv, part_send, part_recv = refs[31:]
    g = Gather(sizes, (mixed, hide, show, stage), (send_sem, recv_sem))
    rows, width = tokens.shape
    groups, cells, local = pool_near.shape
    depth = value_near.shape[0]
    half, block = rows // 2, rows // 12
    inner = hidden.shape[1]
    member, rep, place = g.tp, g.rep, g.place
    nm, nh = g.nm, g.nh
    last = nm + nh
    show_phase = last // 2
    each_group = nm // 2

    loads = [
        pltpu.make_async_copy(far, near, load_sem.at[i])
        for i, (far, near) in enumerate(
            (
                (value_far, value_near),
                (gate_far, gate_near),
                (pool_far, pool_near),
                (tokens_far, tokens),
                (up_far, up_near),
                (down_far, down_near),
            )
        )
    ]

    def remote(source, target, send, recv):
        return pltpu.make_async_remote_copy(
            src_ref=source,
            dst_ref=target,
            send_sem=send,
            recv_sem=recv,
            device_id=g.partner(),
            device_id_type=pl.DeviceIdType.MESH,
        )

    def swap(j, part):
        size = stage.shape[1] // 2
        cut = pl.ds(pl.multiple_of(part * size, 16), size)
        return remote(
            stage.at[2 * (1 - member) + j, cut, :],
            mixed.at[2 * j + member, place, cut, :],
            swap_send.at[j, part],
            swap_recv.at[j, part],
        )

    def keep(j):
        return pltpu.make_async_copy(stage.at[2 * member + j], mixed.at[2 * j + member, place], keep_sem.at[j])

    def merged_copy(slab):
        return remote(merged.at[slab], merged_in.at[slab], pair_send.at[slab], pair_recv.at[slab])

    def part_copy(k, c):
        return remote(parts.at[0, k, c], part_in.at[k, c], part_send.at[k, c], part_recv.at[k, c])

    def round_mixed(group):
        stage[group, :depth, :local] = (value_near[:, group, :] * value_scale[group : group + 1]).astype(jnp.bfloat16)
        stage[group, :depth, local:] = (gate_near[:, group, :] * gate_scale[group : group + 1]).astype(jnp.bfloat16)
        for i in range(2):
            chunk = pool_near[group, i * (cells // 2) : (i + 1) * (cells // 2), :] * pool_scale[group : group + 1]
            stage[group, depth:, i * local : (i + 1) * local] = chunk.astype(jnp.bfloat16)

    def round_up(c):
        wide = hide.shape[3]
        cut = slice(c * wide, (c + 1) * wide)
        hide[c, place] = (up_near[:, cut] * up_scale[:, cut]).astype(jnp.bfloat16)

    def round_down(i):
        part = inner // 4
        at = pl.ds(i * part, part)
        side = show.shape[3]
        for c in range(2):
            cut = slice(c * side, (c + 1) * side)
            show[place, c, at, :] = (down_near[at, cut] * down_scale[:, cut]).astype(jnp.bfloat16)

    def norm_in(part, parts):
        steps = rows // block // parts

        @pl.loop(part * steps, (part + 1) * steps)
        def _(i):
            at = pl.ds(pl.multiple_of(i * block, block), block)
            normed[at, :] = norm_rows(tokens[at, :], mixer_gain[...]).astype(jnp.bfloat16)

    def slab_of(j, q):
        return 2 * j + (member if q == 0 else 1 - member)

    def value_piece(j, q):
        slab = slab_of(j, q)
        weight = mixed[slab, :, :depth, :local].reshape(width, local)

        @pl.loop(0, 2)
        def _(i):
            at = pl.ds(pl.multiple_of(i * half, half), half)
            value = jnp.dot(normed[at, :], weight, preferred_element_type=jnp.float32)
            excess[slab - 2 * j, at, :] = value.astype(jnp.bfloat16)

    def spread_piece(j, q):
        slab = slab_of(j, q)
        group = each_group * member + j
        window = jnp.int32(2)
        for level in range(groups - 1):
            window = jnp.where(group > level, 2 ** (level + 2), window)
        lanes = local // 2

        @pl.loop(0, 2)
        def _(i):
            cut = pl.ds(pl.multiple_of(i * lanes, lanes), lanes)
            floats = excess[slab - 2 * j, :, cut].astype(jnp.float32)
            position = lax.broadcasted_iota(jnp.int32, floats.shape, 0)
            running = floats
            for level in range(groups - each_group + j + 1):
                shifted = pltpu.roll(running, 2**level, 0)
                start = jnp.where(level <= group, 2**level, rows)
                running = running + jnp.where(position >= start, shifted, 0.0)
            counts = jnp.minimum(position + 1, window).astype(jnp.float32)
            excess[slab - 2 * j, :, cut] = (running / counts - floats).astype(jnp.bfloat16)

    def gate_piece(j, q):
        slab = slab_of(j, q)
        gate_weight = mixed[slab, :, :depth, local:].reshape(width, local)
        chunks = [mixed[slab, :, depth:, i * local : (i + 1) * local] for i in range(2)]
        pool = jnp.concatenate(chunks, axis=1).reshape(2 * local, local)

        @pl.loop(0, 2)
        def _(i):
            at = pl.ds(pl.multiple_of(i * half, half), half)
            gate = jnp.dot(normed[at, :], gate_weight, preferred_element_type=jnp.float32)
            pooled = jnp.dot(excess[0, at, :], pool[:local], preferred_element_type=jnp.float32) + jnp.dot(
                excess[1, at, :], pool[local:], preferred_element_type=jnp.float32
            )
            merged[slab, at, :] = (jax.nn.sigmoid(gate) * pooled).astype(jnp.bfloat16)

        merged_copy(slab).start()

    def norm_mid(part, parts):
        if part == 0:
            for slab in range(nm):
                merged_copy(slab).wait_recv()
        steps = rows // block // parts

        @pl.loop(part * steps, (part + 1) * steps)
        def _(i):
            at = pl.ds(pl.multiple_of(i * block, block), block)
            held = []
            for slab in range(nm):
                for source, owner in ((merged, member), (merged_in, 1 - member)):
                    cut = pl.ds(pl.multiple_of((nm * owner + slab) * local, local), local)
                    held.append((cut, tokens[at, cut].astype(jnp.float32) + source[slab, at, :].astype(jnp.float32)))
            total = sum(jnp.sum(values * values, axis=-1, keepdims=True) for _, values in held)
            factor = lax.rsqrt(total / width + 1e-06)
            for cut, values in held:
                normed[at, cut] = (values * factor * channel_gain[:, cut]).astype(jnp.bfloat16)

    def up_piece(c, i):
        weight = hide[c, :, :, i * local : (i + 1) * local].reshape(width, local)
        first = c * hide.shape[3] + i * local

        @pl.loop(0, 2)
        def _(b):
            at = pl.ds(pl.multiple_of(b * half, half), half)
            upward = jnp.dot(normed[at, :], weight, preferred_element_type=jnp.float32)
            hidden[at, first : first + local] = jnp.square(jax.nn.relu(upward)).astype(jnp.bfloat16)

    def down_step(k, c):
        @pl.loop(0, 2)
        def _(b):
            first = lax.rem(b + member + 1, 2) * half
            at = pl.ds(pl.multiple_of(first, half), half)
            part = jnp.dot(hidden[at, :], show[k, c], preferred_element_type=jnp.float32)
            parts[b, k, c] = part.astype(jnp.bfloat16)
            pl.when(b == 0)(lambda: part_copy(k, c).start())

    def down_at(d, column, c):
        if d == 0:
            k = g.z * NY + column
            if column is not g.y:
                g.wait_sibling(show_phase + c, k)
            down_step(k, c)
            return

        @pl.loop(0, 2)
        def _(way):
            zs = g.z - (2 * way - 1) * d

            @pl.when(g.inside(zs))
            def _():
                k = zs * NY + column
                g.wait_sibling(show_phase + c, k)
                down_step(k, c)

    def finish(k):
        side = show.shape[3]
        for c in range(2):
            part_copy(k, c).wait_recv()
            cut = pl.ds(pl.multiple_of((2 * k + c) * side, side), side)
            summed = parts[1, k, c].astype(jnp.float32) + part_in[k, c].astype(jnp.float32)
            out[:, cut] = (middle_of(k, c) + summed).astype(out.dtype)

    def finish_at(d, column):
        @pl.loop(0, 1 if d == 0 else 2)
        def _(way):
            zs = g.z - (2 * way - 1) * d
            pl.when(g.inside(zs))(lambda: finish(zs * NY + column))

    def middle_of(k, c):
        owner, slab = k // nm, k % nm
        side = show.shape[3]
        cut = pl.ds(pl.multiple_of((2 * k + c) * side, side), side)
        at = pl.ds(pl.multiple_of(member * half, half), half)
        near = slice(c * side, (c + 1) * side)
        own = merged[slab, at, near].astype(jnp.float32)
        theirs = merged_in[slab, at, near].astype(jnp.float32)
        return tokens[at, cut].astype(jnp.float32) + jnp.where(owner == member, own, theirs)

    work = []

    def emit(n):
        for _ in range(min(n, len(work))):
            work.pop(0)()

    def add(function, *args):
        work.append(functools.partial(function, *args))

    g.greet()
    for load in loads:
        load.start()
    for load in loads[:3]:
        load.wait()
    for group in range(groups):
        round_mixed(group)
    g.meet()
    swap(0, rep).start()
    g.own(0)
    g.own(2)
    for j in range(each_group):
        keep(j).start()
    swap(0, rep).wait_recv()
    g.own(1)
    swap(1, rep).start()
    for j in range(each_group):
        swap(j, 1 - rep).start()

    def mix(j):
        keep(j).wait()
        swap(j, 1 - rep).wait_recv()
        for q in range(2):
            g.ready(2 * j + q)
            add(value_piece, j, q)
            add(spread_piece, j, q)
        for q in range(2):
            add(gate_piece, j, q)

    def lift(c):
        g.ready(nm + c)
        for i in range(hide.shape[3] // local):
            add(up_piece, c, i)

    def load_up():
        loads[4].wait()
        for c in range(nh):
            round_up(c)

    def load_down():
        loads[5].wait()
        for i in range(4):
            round_down(i)

    show_pieces = tuple(range(last, g.count))
    inward = ((4, 5), (6, 7), show_pieces, ())
    outward = ((3, 4), (5, 6), (7,), show_pieces)

    def next_own(phase):
        g.own_out(*outward[phase])
        g.own_in(*inward[phase])

    other = 1 - g.y
    add(load_up)
    add(loads[3].wait)
    for i in range(4):
        add(norm_in, i, 4)
    add(load_down)
    emits = ((3, 1, 1, 1, 1, 0, 0, 2), (2, 1, 1, 0, 0, 0, 0, 2), (2, 1, 1, 0, 0, 0, 0, 0), (0, 2, 2, 2, 1, 1, 0, 0))
    far = g.nz - 1
    for phase in range(show_phase):
        counts = emits[phase]
        if phase == show_phase - 1:
            for i in range(4):
                add(norm_mid, i, 4)
        g.along(phase, 1)
        if phase == 0:
            swap(1, rep).wait_recv()
            g.own_in(3)
        emit(counts[0])
        g.facing(phase)
        emit(counts[1])
        g.along(phase, 2)
        g.across(phase, 1, True)
        emit(counts[2])
        g.along(phase, 3)
        g.across(phase, 2, True)
        next_own(phase)
        if phase == show_phase - 1:
            for c in range(nh - 2):
                lift(c)
        emit(counts[3])
        g.across(phase, 1, False)
        emit(counts[4])
        g.across(phase, 2, False)
        emit(counts[5])
        g.across(phase, 3, True)
        emit(counts[6])
        g.across(phase, 3, False)
        if phase < each_group:
            mix(phase)
        emit(counts[7])
        if phase == 1:
            add(g.drain, 0)
        elif phase == 2:
            g.drain(1)
    first, second = show_phase, show_phase + 1
    lift(nh - 2)
    lift(nh - 1)
    emit(len(work) - 4)
    g.along(first, 1)
    emit(len(work) - 1)
    g.along(second, 1)
    emit(len(work))
    g.facing(first)
    down_at(0, g.y, 0)
    down_at(0, g.y, 1)
    g.facing(second)
    g.drain(2)
    down_at(1, g.y, 0)
    g.along(first, 2)
    g.across(first, 1, True)
    down_at(0, other, 0)
    down_at(1, g.y, 1)
    g.drain(3)
    down_at(0, other, 1)
    g.across(first, 1, False)
    down_at(2, g.y, 0)
    g.along(second, 2)
    g.across(second, 1, True)
    down_at(1, other, 0)
    g.across(second, 1, False)
    down_at(2, g.y, 1)
    g.along(first, 3)
    g.across(first, 2, True)
    down_at(1, other, 1)
    g.across(first, 2, False)
    down_at(3, g.y, 0)
    g.along(second, 3)
    g.across(second, 2, True)
    down_at(2, other, 0)
    finish_at(0, g.y)
    g.across(second, 2, False)
    down_at(3, g.y, 1)
    finish_at(1, g.y)
    g.across(first, 3, True)
    g.across(first, 3, False)
    down_at(2, other, 1)
    finish_at(0, other)
    g.across(second, 3, True)
    g.across(second, 3, False)
    down_at(3, other, 0)
    down_at(3, other, 1)
    finish_at(2, g.y)
    finish_at(1, other)
    g.drain(first)
    for j in range(each_group):
        for part in range(2):
            swap(j, part).wait_send()
    for slab in range(nm):
        merged_copy(slab).wait_send()
    g.drain(second)
    finish_at(far, g.y)
    finish_at(2, other)
    finish_at(far, other)

    @pl.loop(0, g.nf)
    def _(k):
        for c in range(2):
            part_copy(k, c).wait_send()


def run_layer(sizes, vectors, arrays):
    tokens, value, gate, pool, up, down = arrays
    rows, width = tokens.shape
    depth, groups, local = value.shape
    cells = pool.shape[1]
    inner, wide = down.shape
    nf = sizes["fs"]
    vmem = lambda dims, kind=jnp.bfloat16: pltpu.VMEM(tuple(dims), kind)
    halves = (nf, 2, rows // 2, wide // 2)
    count = 12
    sems = [
        pltpu.SemaphoreType.DMA((4, count, nf)),
        pltpu.SemaphoreType.DMA((2, count, nf)),
        pltpu.SemaphoreType.DMA((len(arrays),)),
        pltpu.SemaphoreType.DMA((2, 2)),
        pltpu.SemaphoreType.DMA((2, 2)),
        pltpu.SemaphoreType.DMA((2,)),
        pltpu.SemaphoreType.DMA((groups,)),
        pltpu.SemaphoreType.DMA((groups,)),
        pltpu.SemaphoreType.DMA((nf, 2)),
        pltpu.SemaphoreType.DMA((nf, 2)),
    ]
    kernel = lambda *refs: pl.run_scoped(functools.partial(layer_kernel, sizes, *refs), *sems)
    return pl.pallas_call(
        kernel,
        out_shape=pltpu.VMEM((rows // 2, width), jnp.bfloat16),
        in_specs=[pl.BlockSpec(memory_space=pltpu.VMEM)] * len(vectors)
        + [pl.BlockSpec(memory_space=pl.ANY)] * len(arrays),
        out_specs=pl.BlockSpec(memory_space=pltpu.VMEM),
        scratch_shapes=[
            vmem((groups, nf, depth + cells // 2, 2 * local)),
            vmem((inner // (2 * local), nf, depth, 2 * local)),
            vmem((nf, 2, inner, wide // 2)),
            vmem((groups, depth + cells // 2, 2 * local)),
            vmem(tokens.shape),
        ]
        + [vmem(array.shape, array.dtype) for array in arrays[1:]]
        + [
            vmem((rows, width)),
            vmem((2, rows, local)),
            vmem((groups, rows, local)),
            vmem((groups, rows, local)),
            vmem((rows, inner)),
            vmem((2, *halves)),
            vmem(halves),
        ],
        compiler_params=pltpu.CompilerParams(
            collective_id=0, has_side_effects=True, vmem_limit_bytes=58 * 2**20
        ),
    )(*vectors, *arrays)


def norm_rows(values, gain):
    floats = values.astype(jnp.float32)
    return floats * lax.rsqrt(jnp.mean(floats * floats, axis=-1, keepdims=True) + 1e-06) * gain


def pool_excess(value):
    floats = value.astype(jnp.float32)
    seq_length = floats.shape[1]
    running = floats
    results = []
    for group in range(floats.shape[2]):
        span = 2**group
        shifted = jnp.pad(running, ((0, 0), (span, 0), (0, 0), (0, 0)))[:, :seq_length]
        running = running + shifted
        counts = jnp.minimum(jnp.arange(1, seq_length + 1), 2 * span).astype(jnp.float32)
        results.append(running[:, :, group, :] / counts[None, :, None] - floats[:, :, group, :])
    return jnp.stack(results, axis=2)


def per_device(
    tokens,
    mixer_gain,
    value_weight,
    value_scale,
    gate_weight,
    gate_scale,
    pool_weight,
    pool_scale,
    channel_gain,
    up_weight,
    up_scale,
    down_weight,
    down_scale,
):
    seq_count, seq_length, model_width = tokens.shape
    shares = lax.axis_size("tp")
    member = lax.axis_index("tp")
    kept_rows = seq_length // shares
    row_count = seq_count * seq_length
    group_count, local_width = value_scale.shape
    value_full, gate_full, pool_full = (
        lax.all_gather(value_weight.astype(jnp.bfloat16), "fs", axis=0, tiled=True),
        lax.all_gather(gate_weight.astype(jnp.bfloat16), "fs", axis=0, tiled=True),
        lax.all_gather(pool_weight.astype(jnp.bfloat16), "fs", axis=1, tiled=True),
    )
    down_scales = lax.all_gather(down_scale, "fs", axis=0, tiled=True)
    normed = norm_rows(tokens, mixer_gain).astype(jnp.bfloat16).reshape(row_count, model_width)
    value = jnp.dot(normed, value_full.reshape(model_width, -1), preferred_element_type=jnp.float32)
    value = (
        (value * value_scale.reshape(-1))
        .astype(jnp.bfloat16)
        .reshape(seq_count, seq_length, group_count, local_width)
    )
    gating = jnp.dot(normed, gate_full.reshape(model_width, -1), preferred_element_type=jnp.float32)
    gating = (gating * gate_scale.reshape(-1)).reshape(
        seq_count, seq_length, group_count, local_width
    )
    excess = pool_excess(value).astype(jnp.bfloat16)
    rows_part = pool_full
    pooled = jnp.einsum(
        "slgc,gce->slge",
        lax.all_gather(excess, "tp", axis=3, tiled=True),
        rows_part,
        preferred_element_type=jnp.float32,
    )
    merged = (jax.nn.sigmoid(gating) * (pooled * pool_scale)).astype(jnp.bfloat16)
    merged_own = lax.all_to_all(merged, "tp", split_axis=1, concat_axis=3, tiled=True)
    own_rows = lax.dynamic_slice_in_dim(tokens, member * kept_rows, kept_rows, 1)
    middle = own_rows.reshape(seq_count * kept_rows, model_width).astype(
        jnp.float32
    ) + merged_own.reshape(seq_count * kept_rows, model_width).astype(jnp.float32)
    normed_two = norm_rows(middle, channel_gain).astype(jnp.bfloat16)
    up_full, down_full = (
        lax.all_gather(up_weight.astype(jnp.bfloat16), "fs", axis=0, tiled=True),
        lax.all_gather(down_weight.astype(jnp.bfloat16), "fs", axis=1, tiled=True),
    )
    upward = (
        jnp.dot(
            lax.all_gather(normed_two, "tp", axis=0, tiled=True),
            up_full,
            preferred_element_type=jnp.float32,
        )
        * up_scale
    )
    hidden = jnp.square(jax.nn.relu(upward)).astype(jnp.bfloat16)
    rows_part = hidden
    summed = lax.psum_scatter(
        (jnp.dot(rows_part, down_full, preferred_element_type=jnp.float32) * down_scales).astype(
            jnp.bfloat16
        ),
        "tp",
        scatter_dimension=0,
        tiled=True,
    ).astype(jnp.float32)
    return (middle + summed).astype(jnp.bfloat16).reshape(seq_count, kept_rows, model_width)


def paired_device(
    sizes,
    tokens,
    mixer_gain,
    value_weight,
    value_scale,
    gate_weight,
    gate_scale,
    pool_weight,
    pool_scale,
    channel_gain,
    up_weight,
    up_scale,
    down_weight,
    down_scale,
):
    row = lambda vector: vector.reshape(1, -1)
    out = run_layer(
        sizes,
        (row(mixer_gain), value_scale, gate_scale, pool_scale, row(channel_gain), row(up_scale), row(down_scale)),
        (tokens[0], value_weight, gate_weight, pool_weight, up_weight, down_weight),
    )
    return out[None]


def solution(mesh):
    sizes = dict(mesh.shape)
    paired = sizes["rep"] == 2 and sizes["tp"] == 2 and sizes["fs"] == 8

    def body(tokens, *rest):
        value_scale, down_scale = rest[2], rest[-1]
        square = value_scale.shape[1] == down_scale.shape[0] == rest[1].shape[0]
        if paired and tokens.shape[0] == 1 and square and value_scale.shape[0] == 4:
            return paired_device(sizes, tokens, *rest)
        return per_device(tokens, *rest)

    return jax.shard_map(
        body,
        mesh=mesh,
        in_specs=(
            P(("rep", "fs"), None, None),
            P(),
            P("fs", None, "tp"),
            P(None, "tp"),
            P("fs", None, "tp"),
            P(None, "tp"),
            P(None, "fs", "tp"),
            P(None, "tp"),
            P(),
            P("fs", "tp"),
            P("tp"),
            P("tp", "fs"),
            P("fs"),
        ),
        out_specs=P(("rep", "fs"), "tp", None),
        check_vma=False,
    )
```

```python
import functools

import jax
import jax.numpy as jnp
from jax import lax
from jax.experimental import pallas as pl
from jax.experimental.pallas import tpu as pltpu
from jax.sharding import PartitionSpec as P

NY = 2
ACROSS, SIBLING = 2, 3


class Gather:
    def __init__(self, sizes, bufs, sems):
        self.nf = sizes["fs"]
        self.nz = self.nf // NY
        self.rep, self.place, self.tp = lax.axis_index("rep"), lax.axis_index("fs"), lax.axis_index("tp")
        self.z, self.y = self.place // NY, self.place % NY
        self.mixed, self.hide, self.show, self.stage = bufs
        self.send_sem, self.recv_sem = sems
        self.nm, self.nh = self.mixed.shape[0], self.hide.shape[0]
        self.subs = 4
        self.count = self.nm + self.nh + self.subs

    def device(self, way):
        rep, place = self.rep, self.place
        if isinstance(way, int) and way == ACROSS:
            place = self.z * NY + 1 - self.y
        elif isinstance(way, int) and way == SIBLING:
            rep = 1 - rep
        else:
            place = place + NY * (2 * way - 1)
        return {"rep": rep, "fs": place, "tp": self.tp}

    def partner(self):
        return {"rep": self.rep, "fs": self.place, "tp": 1 - self.tp}

    def half_of(self, p):
        j, q = p // 2, p % 2
        return 2 * j + (self.tp if q == 0 else 1 - self.tp)

    def piece(self, p, k, half):
        if p < self.nm:
            part = self.mixed.shape[2] // 2
            return self.mixed.at[self.half_of(p), k, pl.ds(pl.multiple_of(half * part, 16), part), :]
        if p < self.nm + self.nh:
            part = self.hide.shape[2] // 2
            return self.hide.at[p - self.nm, k, pl.ds(pl.multiple_of(half * part, 16), part), :]
        part = self.show.shape[2] // 4
        side, deep = (p - self.nm - self.nh) // 2, p % 2
        return self.show.at[k, side, pl.ds(pl.multiple_of((2 * deep + half) * part, 16), part), :]

    def copy(self, p, k, way, half=None, src=None):
        half = self.rep if half is None else half
        sibling = isinstance(way, int) and way == SIBLING
        return pltpu.make_async_remote_copy(
            src_ref=self.piece(p, k, half) if src is None else src,
            dst_ref=self.piece(p, k, half),
            send_sem=self.send_sem.at[way, p, k],
            recv_sem=self.recv_sem.at[1 if sibling else 0, p, k],
            device_id=self.device(way),
            device_id_type=pl.DeviceIdType.MESH,
        )

    def inside(self, z):
        return (z >= 0) & (z < self.nz)

    def wide(self, p, zs):
        return ((zs == 0) | (zs == self.nz - 1)) & (self.rep == p % 2)

    def greet(self):
        sem = pltpu.get_barrier_semaphore()

        def signal(device):
            pl.semaphore_signal(sem, inc=1, device_id=device, device_id_type=pl.DeviceIdType.MESH)

        signal(self.device(ACROSS))
        signal(self.device(SIBLING))
        signal(self.partner())
        pl.when(self.z > 0)(lambda: signal(self.device(0)))
        pl.when(self.z < self.nz - 1)(lambda: signal(self.device(1)))

    def meet(self):
        ends = (self.z > 0).astype(jnp.int32) + (self.z < self.nz - 1).astype(jnp.int32)
        pl.semaphore_wait(pltpu.get_barrier_semaphore(), 3 + ends)

    def each(self, phase, body):
        for p in (2 * phase, 2 * phase + 1):
            body(p)

    def source(self, p):
        if p >= self.nm or p % 2:
            return None
        part = self.stage.shape[1] // 2
        rows = pl.ds(pl.multiple_of(self.rep * part, 16), part)
        return self.stage.at[2 * self.tp + p // 2, rows, :]

    def own_in(self, *pieces):
        for p in pieces:
            src = self.source(p)
            way = (self.z == 0).astype(jnp.int32)
            end = (self.z == 0) | (self.z == self.nz - 1)
            pl.when(end)(lambda: self.copy(p, self.place, way, src=src).start())

    def own_out(self, *pieces):
        for p in pieces:
            src = self.source(p)

            @pl.when((self.z > 0) & (self.z < self.nz - 1))
            def _():
                for way in range(2):
                    self.copy(p, self.place, way, src=src).start()

            self.copy(p, self.place, ACROSS, src=src).start()

    def own(self, *pieces):
        self.own_in(*pieces)
        self.own_out(*pieces)

    def along(self, phase, d):
        @pl.loop(0, 2)
        def _(way):
            step = 2 * way - 1
            zs = self.z - step * d

            @pl.when(self.inside(zs))
            def _():
                k = zs * NY + self.y

                def body(p):
                    self.copy(p, k, ACROSS).wait_recv()
                    pl.when(self.inside(self.z + step))(lambda: self.copy(p, k, way).start())
                    pl.when(jnp.logical_not(self.wide(p, zs)))(lambda: self.copy(p, k, ACROSS).start())
                    self.copy(p, k, SIBLING).start()

                self.each(phase, body)

    def facing(self, phase):
        k = self.z * NY + 1 - self.y
        way = (self.z == 0).astype(jnp.int32)

        def body(p):
            self.copy(p, k, ACROSS).wait_recv()
            pl.when(self.wide(p, self.z))(lambda: self.copy(p, k, way).start())
            self.copy(p, k, SIBLING).start()

        self.each(phase, body)

    def across(self, phase, d, wide):
        @pl.loop(0, 2)
        def _(way):
            step = 2 * way - 1
            zs = self.z - step * d
            k = zs * NY + 1 - self.y

            def body(p):
                @pl.when(self.wide(p, zs) if wide else jnp.logical_not(self.wide(p, zs)))
                def _():
                    self.copy(p, k, ACROSS).wait_recv()
                    if wide:
                        pl.when(self.inside(self.z + step))(lambda: self.copy(p, k, way).start())
                    self.copy(p, k, SIBLING).start()

            pl.when(self.inside(zs))(lambda: self.each(phase, body))

    def wait_sibling(self, phase, k):
        self.each(phase, lambda p: self.copy(p, k, SIBLING, half=1 - self.rep).wait_recv())

    def ready(self, p):
        @pl.loop(0, self.nf)
        def _(k):
            pl.when(k != self.place)(lambda: self.copy(p, k, SIBLING, half=1 - self.rep).wait_recv())

    def drain(self, phase):
        def body(p):
            src = self.source(p)

            @pl.loop(0, self.nf)
            def _(k):
                zs, mine = k // NY, k % NY == self.y
                wide = self.wide(p, zs)
                here = zs == self.z

                @pl.loop(0, 2)
                def _(way):
                    step = 2 * way - 1
                    away = here | (step * (self.z - zs) > 0)
                    sent = self.inside(self.z + step) & away & (mine | wide)
                    pl.when(sent)(lambda: self.copy(p, k, way).wait_send())

                pl.when(mine & (here | jnp.logical_not(wide)))(lambda: self.copy(p, k, ACROSS).wait_send())
                pl.when(k != self.place)(lambda: self.copy(p, k, SIBLING).wait_send())

        self.each(phase, body)


def layer_kernel(sizes, *refs):
    vectors_far, vectors = refs[:7], refs[31:38]
    mixer_gain, value_scale, gate_scale, pool_scale, channel_gain, up_scale, down_scale = vectors
    tokens_far, value_far, gate_far, pool_far, up_far, down_far, out = refs[7:14]
    mixed, hide, show, stage = refs[14:18]
    tokens, value_near, gate_near, pool_near, up_near, down_near = refs[18:24]
    normed, excess, merged, merged_in, hidden, parts, part_in = refs[24:31]
    send_sem, recv_sem, load_sem, swap_send, swap_recv, keep_sem, pair_send, pair_recv, part_send, part_recv = refs[38:]
    g = Gather(sizes, (mixed, hide, show, stage), (send_sem, recv_sem))
    rows, width = tokens.shape
    groups, cells, local = pool_near.shape
    depth = value_near.shape[0]
    half, block = rows // 2, rows // 12
    inner = hidden.shape[1]
    member, rep, place = g.tp, g.rep, g.place
    nm, nh = g.nm, g.nh
    last = nm + nh
    show_phase = last // 2
    each_group = nm // 2

    loads = [
        pltpu.make_async_copy(far, near, load_sem.at[i])
        for i, (far, near) in enumerate(
            (
                (value_far, value_near),
                (gate_far, gate_near),
                (pool_far, pool_near),
                (tokens_far, tokens),
                (up_far, up_near),
                (down_far, down_near),
            )
        )
    ]

    small = [
        pltpu.make_async_copy(far, near, load_sem.at[len(loads) + i])
        for i, (far, near) in enumerate(zip(vectors_far, vectors))
    ]

    def remote(source, target, send, recv):
        return pltpu.make_async_remote_copy(
            src_ref=source,
            dst_ref=target,
            send_sem=send,
            recv_sem=recv,
            device_id=g.partner(),
            device_id_type=pl.DeviceIdType.MESH,
        )

    def swap(j, part):
        size = stage.shape[1] // 2
        cut = pl.ds(pl.multiple_of(part * size, 16), size)
        return remote(
            stage.at[2 * (1 - member) + j, cut, :],
            mixed.at[2 * j + member, place, cut, :],
            swap_send.at[j, part],
            swap_recv.at[j, part],
        )

    def keep(j):
        return pltpu.make_async_copy(stage.at[2 * member + j], mixed.at[2 * j + member, place], keep_sem.at[j])

    def merged_copy(slab):
        return remote(merged.at[slab], merged_in.at[slab], pair_send.at[slab], pair_recv.at[slab])

    def part_copy(k, c):
        return remote(parts.at[0, k, c], part_in.at[k, c], part_send.at[k, c], part_recv.at[k, c])

    def round_mixed(group):
        stage[group, :depth, :local] = (value_near[:, group, :] * value_scale[group : group + 1]).astype(jnp.bfloat16)
        stage[group, :depth, local:] = (gate_near[:, group, :] * gate_scale[group : group + 1]).astype(jnp.bfloat16)
        for i in range(2):
            chunk = pool_near[group, i * (cells // 2) : (i + 1) * (cells // 2), :] * pool_scale[group : group + 1]
            stage[group, depth:, i * local : (i + 1) * local] = chunk.astype(jnp.bfloat16)

    def round_up(c):
        wide = hide.shape[3]
        cut = slice(c * wide, (c + 1) * wide)
        hide[c, place] = (up_near[:, cut] * up_scale[:, cut]).astype(jnp.bfloat16)

    def round_down(i):
        part = inner // 4
        at = pl.ds(i * part, part)
        side = show.shape[3]
        for c in range(2):
            cut = slice(c * side, (c + 1) * side)
            show[place, c, at, :] = (down_near[at, cut] * down_scale[:, cut]).astype(jnp.bfloat16)

    def norm_in(part, parts):
        steps = rows // block // parts

        @pl.loop(part * steps, (part + 1) * steps)
        def _(i):
            at = pl.ds(pl.multiple_of(i * block, block), block)
            normed[at, :] = norm_rows(tokens[at, :], mixer_gain[...]).astype(jnp.bfloat16)

    def slab_of(j, q):
        return 2 * j + (member if q == 0 else 1 - member)

    def value_piece(j, q):
        slab = slab_of(j, q)
        weight = mixed[slab, :, :depth, :local].reshape(width, local)

        @pl.loop(0, 2)
        def _(i):
            at = pl.ds(pl.multiple_of(i * half, half), half)
            value = jnp.dot(normed[at, :], weight, preferred_element_type=jnp.float32)
            excess[slab - 2 * j, at, :] = value.astype(jnp.bfloat16)

    def spread_piece(j, q):
        slab = slab_of(j, q)
        group = each_group * member + j
        window = jnp.int32(2)
        for level in range(groups - 1):
            window = jnp.where(group > level, 2 ** (level + 2), window)
        lanes = local // 2

        @pl.loop(0, 2)
        def _(i):
            cut = pl.ds(pl.multiple_of(i * lanes, lanes), lanes)
            floats = excess[slab - 2 * j, :, cut].astype(jnp.float32)
            position = lax.broadcasted_iota(jnp.int32, floats.shape, 0)
            running = floats
            for level in range(groups - each_group + j + 1):
                shifted = pltpu.roll(running, 2**level, 0)
                start = jnp.where(level <= group, 2**level, rows)
                running = running + jnp.where(position >= start, shifted, 0.0)
            counts = jnp.minimum(position + 1, window).astype(jnp.float32)
            excess[slab - 2 * j, :, cut] = (running / counts - floats).astype(jnp.bfloat16)

    def gate_piece(j, q):
        slab = slab_of(j, q)
        gate_weight = mixed[slab, :, :depth, local:].reshape(width, local)
        chunks = [mixed[slab, :, depth:, i * local : (i + 1) * local] for i in range(2)]
        pool = jnp.concatenate(chunks, axis=1).reshape(2 * local, local)

        @pl.loop(0, 2)
        def _(i):
            at = pl.ds(pl.multiple_of(i * half, half), half)
            gate = jnp.dot(normed[at, :], gate_weight, preferred_element_type=jnp.float32)
            pooled = jnp.dot(excess[0, at, :], pool[:local], preferred_element_type=jnp.float32) + jnp.dot(
                excess[1, at, :], pool[local:], preferred_element_type=jnp.float32
            )
            merged[slab, at, :] = (jax.nn.sigmoid(gate) * pooled).astype(jnp.bfloat16)

        merged_copy(slab).start()

    def norm_mid(part, parts):
        if part == 0:
            for slab in range(nm):
                merged_copy(slab).wait_recv()
        steps = rows // block // parts

        @pl.loop(part * steps, (part + 1) * steps)
        def _(i):
            at = pl.ds(pl.multiple_of(i * block, block), block)
            held = []
            for slab in range(nm):
                for source, owner in ((merged, member), (merged_in, 1 - member)):
                    cut = pl.ds(pl.multiple_of((nm * owner + slab) * local, local), local)
                    held.append((cut, tokens[at, cut].astype(jnp.float32) + source[slab, at, :].astype(jnp.float32)))
            total = sum(jnp.sum(values * values, axis=-1, keepdims=True) for _, values in held)
            factor = lax.rsqrt(total / width + 1e-06)
            for cut, values in held:
                normed[at, cut] = (values * factor * channel_gain[:, cut]).astype(jnp.bfloat16)

    def up_piece(c, i):
        weight = hide[c, :, :, i * local : (i + 1) * local].reshape(width, local)
        first = c * hide.shape[3] + i * local

        @pl.loop(0, 2)
        def _(b):
            at = pl.ds(pl.multiple_of(b * half, half), half)
            upward = jnp.dot(normed[at, :], weight, preferred_element_type=jnp.float32)
            hidden[at, first : first + local] = jnp.square(jax.nn.relu(upward)).astype(jnp.bfloat16)

    def down_step(k, c):
        @pl.loop(0, 2)
        def _(b):
            first = lax.rem(b + member + 1, 2) * half
            at = pl.ds(pl.multiple_of(first, half), half)
            part = jnp.dot(hidden[at, :], show[k, c], preferred_element_type=jnp.float32)
            parts[b, k, c] = part.astype(jnp.bfloat16)
            pl.when(b == 0)(lambda: part_copy(k, c).start())

    def down_at(d, column, c):
        if d == 0:
            k = g.z * NY + column
            if column is not g.y:
                g.wait_sibling(show_phase + c, k)
            down_step(k, c)
            return

        @pl.loop(0, 2)
        def _(way):
            zs = g.z - (2 * way - 1) * d

            @pl.when(g.inside(zs))
            def _():
                k = zs * NY + column
                g.wait_sibling(show_phase + c, k)
                down_step(k, c)

    def finish(k):
        side = show.shape[3]
        for c in range(2):
            part_copy(k, c).wait_recv()
            cut = pl.ds(pl.multiple_of((2 * k + c) * side, side), side)
            summed = parts[1, k, c].astype(jnp.float32) + part_in[k, c].astype(jnp.float32)
            out[:, cut] = (middle_of(k, c) + summed).astype(out.dtype)

    def finish_at(d, column):
        @pl.loop(0, 1 if d == 0 else 2)
        def _(way):
            zs = g.z - (2 * way - 1) * d
            pl.when(g.inside(zs))(lambda: finish(zs * NY + column))

    def middle_of(k, c):
        owner, slab = k // nm, k % nm
        side = show.shape[3]
        cut = pl.ds(pl.multiple_of((2 * k + c) * side, side), side)
        at = pl.ds(pl.multiple_of(member * half, half), half)
        near = slice(c * side, (c + 1) * side)
        own = merged[slab, at, near].astype(jnp.float32)
        theirs = merged_in[slab, at, near].astype(jnp.float32)
        return tokens[at, cut].astype(jnp.float32) + jnp.where(owner == member, own, theirs)

    work = []

    def emit(n):
        for _ in range(min(n, len(work))):
            work.pop(0)()

    def add(function, *args):
        work.append(functools.partial(function, *args))

    g.greet()
    for load in loads[:3] + small:
        load.start()
    for load in loads[:3] + small:
        load.wait()
    for group in range(groups):
        round_mixed(group)
    g.meet()
    swap(0, rep).start()
    g.own(0)
    g.own(2)
    for load in loads[3:]:
        load.start()
    for j in range(each_group):
        keep(j).start()
    swap(0, rep).wait_recv()
    g.own(1)
    swap(1, rep).start()
    for j in range(each_group):
        swap(j, 1 - rep).start()

    def mix(j):
        keep(j).wait()
        swap(j, 1 - rep).wait_recv()
        for q in range(2):
            g.ready(2 * j + q)
            add(value_piece, j, q)
            add(spread_piece, j, q)
        for q in range(2):
            add(gate_piece, j, q)

    def lift(c):
        g.ready(nm + c)
        for i in range(hide.shape[3] // local):
            add(up_piece, c, i)

    def load_up():
        loads[4].wait()
        for c in range(nh):
            round_up(c)

    def load_down():
        loads[5].wait()
        for i in range(4):
            round_down(i)

    show_pieces = tuple(range(last, g.count))
    inward = ((4, 5), (6, 7), show_pieces, ())
    outward = ((3, 4), (5, 6), (7,), show_pieces)

    def next_own(phase):
        g.own_out(*outward[phase])
        g.own_in(*inward[phase])

    other = 1 - g.y
    add(load_up)
    add(loads[3].wait)
    for i in range(4):
        add(norm_in, i, 4)
    add(load_down)
    emits = ((3, 1, 1, 1, 1, 0, 0, 2), (2, 1, 1, 0, 0, 0, 0, 2), (2, 1, 1, 0, 0, 0, 0, 0), (0, 2, 2, 2, 1, 1, 0, 0))
    far = g.nz - 1
    for phase in range(show_phase):
        counts = emits[phase]
        if phase == show_phase - 1:
            for i in range(4):
                add(norm_mid, i, 4)
        g.along(phase, 1)
        if phase == 0:
            swap(1, rep).wait_recv()
            g.own_in(3)
        emit(counts[0])
        g.facing(phase)
        emit(counts[1])
        g.along(phase, 2)
        g.across(phase, 1, True)
        emit(counts[2])
        g.along(phase, 3)
        g.across(phase, 2, True)
        next_own(phase)
        if phase == show_phase - 1:
            for c in range(nh - 2):
                lift(c)
        emit(counts[3])
        g.across(phase, 1, False)
        emit(counts[4])
        g.across(phase, 2, False)
        emit(counts[5])
        g.across(phase, 3, True)
        emit(counts[6])
        g.across(phase, 3, False)
        if phase < each_group:
            mix(phase)
        emit(counts[7])
        if phase == 1:
            add(g.drain, 0)
        elif phase == 2:
            g.drain(1)
    first, second = show_phase, show_phase + 1
    lift(nh - 2)
    lift(nh - 1)
    emit(len(work) - 4)
    g.along(first, 1)
    emit(len(work) - 1)
    g.along(second, 1)
    emit(len(work))
    g.facing(first)
    down_at(0, g.y, 0)
    down_at(0, g.y, 1)
    g.facing(second)
    g.drain(2)
    down_at(1, g.y, 0)
    g.along(first, 2)
    g.across(first, 1, True)
    down_at(0, other, 0)
    down_at(1, g.y, 1)
    g.drain(3)
    down_at(0, other, 1)
    g.across(first, 1, False)
    down_at(2, g.y, 0)
    g.along(second, 2)
    g.across(second, 1, True)
    down_at(1, other, 0)
    g.across(second, 1, False)
    down_at(2, g.y, 1)
    g.along(first, 3)
    g.across(first, 2, True)
    down_at(1, other, 1)
    g.across(first, 2, False)
    down_at(3, g.y, 0)
    g.along(second, 3)
    g.across(second, 2, True)
    down_at(2, other, 0)
    finish_at(0, g.y)
    g.across(second, 2, False)
    down_at(3, g.y, 1)
    finish_at(1, g.y)
    g.across(first, 3, True)
    g.across(first, 3, False)
    down_at(2, other, 1)
    finish_at(0, other)
    g.across(second, 3, True)
    g.across(second, 3, False)
    down_at(3, other, 0)
    down_at(3, other, 1)
    finish_at(2, g.y)
    finish_at(1, other)
    g.drain(first)
    for j in range(each_group):
        for part in range(2):
            swap(j, part).wait_send()
    for slab in range(nm):
        merged_copy(slab).wait_send()
    g.drain(second)
    finish_at(far, g.y)
    finish_at(2, other)
    finish_at(far, other)

    @pl.loop(0, g.nf)
    def _(k):
        for c in range(2):
            part_copy(k, c).wait_send()


def run_layer(sizes, vectors, arrays):
    tokens, value, gate, pool, up, down = arrays
    rows, width = tokens.shape
    depth, groups, local = value.shape
    cells = pool.shape[1]
    inner, wide = down.shape
    nf = sizes["fs"]
    vmem = lambda dims, kind=jnp.bfloat16: pltpu.VMEM(tuple(dims), kind)
    halves = (nf, 2, rows // 2, wide // 2)
    count = 12
    sems = [
        pltpu.SemaphoreType.DMA((4, count, nf)),
        pltpu.SemaphoreType.DMA((2, count, nf)),
        pltpu.SemaphoreType.DMA((len(arrays) + len(vectors),)),
        pltpu.SemaphoreType.DMA((2, 2)),
        pltpu.SemaphoreType.DMA((2, 2)),
        pltpu.SemaphoreType.DMA((2,)),
        pltpu.SemaphoreType.DMA((groups,)),
        pltpu.SemaphoreType.DMA((groups,)),
        pltpu.SemaphoreType.DMA((nf, 2)),
        pltpu.SemaphoreType.DMA((nf, 2)),
    ]
    kernel = lambda *refs: pl.run_scoped(functools.partial(layer_kernel, sizes, *refs), *sems)
    return pl.pallas_call(
        kernel,
        out_shape=pltpu.VMEM((rows // 2, width), jnp.bfloat16),
        in_specs=[pl.BlockSpec(memory_space=pl.ANY)] * (len(vectors) + len(arrays)),
        out_specs=pl.BlockSpec(memory_space=pltpu.VMEM),
        scratch_shapes=[
            vmem((groups, nf, depth + cells // 2, 2 * local)),
            vmem((inner // (2 * local), nf, depth, 2 * local)),
            vmem((nf, 2, inner, wide // 2)),
            vmem((groups, depth + cells // 2, 2 * local)),
            vmem(tokens.shape),
        ]
        + [vmem(array.shape, array.dtype) for array in arrays[1:]]
        + [
            vmem((rows, width)),
            vmem((2, rows, local)),
            vmem((groups, rows, local)),
            vmem((groups, rows, local)),
            vmem((rows, inner)),
            vmem((2, *halves)),
            vmem(halves),
            *[vmem(vector.shape, vector.dtype) for vector in vectors],
        ],
        compiler_params=pltpu.CompilerParams(
            collective_id=0, has_side_effects=True, vmem_limit_bytes=58 * 2**20
        ),
    )(*vectors, *arrays)


def norm_rows(values, gain):
    floats = values.astype(jnp.float32)
    return floats * lax.rsqrt(jnp.mean(floats * floats, axis=-1, keepdims=True) + 1e-06) * gain


def pool_excess(value):
    floats = value.astype(jnp.float32)
    seq_length = floats.shape[1]
    running = floats
    results = []
    for group in range(floats.shape[2]):
        span = 2**group
        shifted = jnp.pad(running, ((0, 0), (span, 0), (0, 0), (0, 0)))[:, :seq_length]
        running = running + shifted
        counts = jnp.minimum(jnp.arange(1, seq_length + 1), 2 * span).astype(jnp.float32)
        results.append(running[:, :, group, :] / counts[None, :, None] - floats[:, :, group, :])
    return jnp.stack(results, axis=2)


def per_device(
    tokens,
    mixer_gain,
    value_weight,
    value_scale,
    gate_weight,
    gate_scale,
    pool_weight,
    pool_scale,
    channel_gain,
    up_weight,
    up_scale,
    down_weight,
    down_scale,
):
    seq_count, seq_length, model_width = tokens.shape
    shares = lax.axis_size("tp")
    member = lax.axis_index("tp")
    kept_rows = seq_length // shares
    row_count = seq_count * seq_length
    group_count, local_width = value_scale.shape
    value_full, gate_full, pool_full = (
        lax.all_gather(value_weight.astype(jnp.bfloat16), "fs", axis=0, tiled=True),
        lax.all_gather(gate_weight.astype(jnp.bfloat16), "fs", axis=0, tiled=True),
        lax.all_gather(pool_weight.astype(jnp.bfloat16), "fs", axis=1, tiled=True),
    )
    down_scales = lax.all_gather(down_scale, "fs", axis=0, tiled=True)
    normed = norm_rows(tokens, mixer_gain).astype(jnp.bfloat16).reshape(row_count, model_width)
    value = jnp.dot(normed, value_full.reshape(model_width, -1), preferred_element_type=jnp.float32)
    value = (
        (value * value_scale.reshape(-1))
        .astype(jnp.bfloat16)
        .reshape(seq_count, seq_length, group_count, local_width)
    )
    gating = jnp.dot(normed, gate_full.reshape(model_width, -1), preferred_element_type=jnp.float32)
    gating = (gating * gate_scale.reshape(-1)).reshape(
        seq_count, seq_length, group_count, local_width
    )
    excess = pool_excess(value).astype(jnp.bfloat16)
    rows_part = pool_full
    pooled = jnp.einsum(
        "slgc,gce->slge",
        lax.all_gather(excess, "tp", axis=3, tiled=True),
        rows_part,
        preferred_element_type=jnp.float32,
    )
    merged = (jax.nn.sigmoid(gating) * (pooled * pool_scale)).astype(jnp.bfloat16)
    merged_own = lax.all_to_all(merged, "tp", split_axis=1, concat_axis=3, tiled=True)
    own_rows = lax.dynamic_slice_in_dim(tokens, member * kept_rows, kept_rows, 1)
    middle = own_rows.reshape(seq_count * kept_rows, model_width).astype(
        jnp.float32
    ) + merged_own.reshape(seq_count * kept_rows, model_width).astype(jnp.float32)
    normed_two = norm_rows(middle, channel_gain).astype(jnp.bfloat16)
    up_full, down_full = (
        lax.all_gather(up_weight.astype(jnp.bfloat16), "fs", axis=0, tiled=True),
        lax.all_gather(down_weight.astype(jnp.bfloat16), "fs", axis=1, tiled=True),
    )
    upward = (
        jnp.dot(
            lax.all_gather(normed_two, "tp", axis=0, tiled=True),
            up_full,
            preferred_element_type=jnp.float32,
        )
        * up_scale
    )
    hidden = jnp.square(jax.nn.relu(upward)).astype(jnp.bfloat16)
    rows_part = hidden
    summed = lax.psum_scatter(
        (jnp.dot(rows_part, down_full, preferred_element_type=jnp.float32) * down_scales).astype(
            jnp.bfloat16
        ),
        "tp",
        scatter_dimension=0,
        tiled=True,
    ).astype(jnp.float32)
    return (middle + summed).astype(jnp.bfloat16).reshape(seq_count, kept_rows, model_width)


def paired_device(
    sizes,
    tokens,
    mixer_gain,
    value_weight,
    value_scale,
    gate_weight,
    gate_scale,
    pool_weight,
    pool_scale,
    channel_gain,
    up_weight,
    up_scale,
    down_weight,
    down_scale,
):
    row = lambda vector: vector.reshape(1, -1)
    out = run_layer(
        sizes,
        (row(mixer_gain), value_scale, gate_scale, pool_scale, row(channel_gain), row(up_scale), row(down_scale)),
        (tokens[0], value_weight, gate_weight, pool_weight, up_weight, down_weight),
    )
    return out[None]


def solution(mesh):
    sizes = dict(mesh.shape)
    paired = sizes["rep"] == 2 and sizes["tp"] == 2 and sizes["fs"] == 8

    def body(tokens, *rest):
        value_scale, down_scale = rest[2], rest[-1]
        square = value_scale.shape[1] == down_scale.shape[0] == rest[1].shape[0]
        if paired and tokens.shape[0] == 1 and square and value_scale.shape[0] == 4:
            return paired_device(sizes, tokens, *rest)
        return per_device(tokens, *rest)

    return jax.shard_map(
        body,
        mesh=mesh,
        in_specs=(
            P(("rep", "fs"), None, None),
            P(),
            P("fs", None, "tp"),
            P(None, "tp"),
            P("fs", None, "tp"),
            P(None, "tp"),
            P(None, "fs", "tp"),
            P(None, "tp"),
            P(),
            P("fs", "tp"),
            P("tp"),
            P("tp", "fs"),
            P("fs"),
        ),
        out_specs=P(("rep", "fs"), "tp", None),
        check_vma=False,
    )
```
